32 devices in a mesh: sp: 4 (over z), fs: 4 (over y, x), tp: 2 (over core).
Axes of the slice: x: 2, y: 2, z: 4, core: 2. Of those that a mesh axis runs over, the one named last changes fastest.
Arguments:
- tokens: bfloat16 [16384, 2048], P(('fs', 'sp', 'tp')), parts along dimension 0, may hold values from -6 to 6
- norm_gain: float32 [2048], replicated, may hold values from 0.1 to 1.9
- w_pool: bfloat16 [2048, 1024], P(None, 'tp'), may hold values from -0.125 to 0.125
- w_query: bfloat16 [2048, 1024], P(None, 'tp'), may hold values from -0.125 to 0.125
- w_key: bfloat16 [2048, 1024], P(None, 'tp'), may hold values from -0.125 to 0.125
- w_value: bfloat16 [2048, 1024], P(None, 'tp'), may hold values from -0.125 to 0.125
- w_gate: bfloat16 [2048, 1024], P(None, 'tp'), may hold values from -0.125 to 0.125
- pool_mix: bfloat16 [4, 256, 256], P('tp'), may hold values from -0.375 to 0.375
- pool_bias: float32 [4, 256], P('tp'), may hold values from -3 to 3
- pool_gain: float32 [1024], P('tp'), may hold values from 0.1 to 1.9
- ret_gain: float32 [1024], P('tp'), may hold values from 0.1 to 1.9
- w_out_pool: bfloat16 [1024, 2048], P('tp'), may hold values from -0.125 to 0.125
- w_out_ret: bfloat16 [1024, 2048], P('tp'), may hold values from -0.125 to 0.125
Outputs:
- mixed: bfloat16 [16384, 2048], P(('fs', 'sp', 'tp')), parts along dimension 0
The draws below stay inside these ranges and needn't reach their ends.
There are 4 independent parts, one for each index of `fs`. The reference program is written for one: setup_inputs(seed, part) draws one part's arguments, and reference() takes and returns one part's arrays. A program takes and returns all parts, laid end to end along the dimension named above; an argument that names none is the same for every part. Nothing has to cross between parts.
All inputs are finite; a program needn't handle non-finite values.
Results may differ from the reference program's by a relative error of at most 0.012.
Values may be sent and summed in bfloat16 or wider, within the bound.
A program may use at most 128 MiB of HBM per device.

```python
import jax
import jax.numpy as jnp
from jax import lax

D = 2048
GROUP_DIM = 256
POOL_WIDTH = 1024
HEADS = 8
HEAD_DIM = 128
RET_WIDTH = 1024
BLOCK = 128
SEQ = 4096
N_TP = 2


def level_of(own_key, shape, cuts, smallest, high):
    factor_of, own = 1.0, jax.random.fold_in(own_key, 6)
    for dim, shards_of in cuts:
        steps = jnp.exp(jax.random.uniform(jax.random.fold_in(own, dim), (shards_of,), jnp.float32, smallest / len(cuts), high / len(cuts)))
        factor_of = factor_of * jnp.repeat(steps, shape[dim] // shards_of).reshape([-1 if axis == dim else 1 for axis in range(len(shape))])
    return factor_of


def noise(rng, extent, width, bound, cuts=(), kind=jnp.bfloat16):
    level = level_of(rng, extent, cuts, -0.22, 0.18) if cuts else 1.0
    entries = jax.random.normal(rng, extent, jnp.float32) * width * level
    return jnp.minimum(jnp.maximum(entries, -bound), bound).astype(kind)


def setup_inputs(seed: int = 0, part: int = 0) -> dict:
    splits = jax.random.split(jax.random.key(seed), 14)
    part_splits = jax.random.split(jax.random.fold_in(splits[13], part), 14)
    return {
        "tokens": noise(part_splits[0], (SEQ, D), 1.0, 6.0, ((0, 8),)),
        "norm_gain": jnp.clip(1.0 + 0.18 * jax.random.normal(splits[1], (D,), jnp.float32), 0.1, 1.9),
        "w_pool": noise(splits[2], (D, POOL_WIDTH), D ** -0.5, 0.125, ((1, 2),)),
        "w_query": noise(splits[3], (D, RET_WIDTH), D ** -0.5, 0.125, ((1, 2),)),
        "w_key": noise(splits[4], (D, RET_WIDTH), D ** -0.5, 0.125, ((1, 2),)),
        "w_value": noise(splits[5], (D, RET_WIDTH), D ** -0.5, 0.125, ((1, 2),)),
        "w_gate": noise(splits[6], (D, RET_WIDTH), D ** -0.5, 0.125, ((1, 2),)),
        "pool_mix": noise(splits[7], (4, GROUP_DIM, GROUP_DIM), GROUP_DIM ** -0.5, 0.375, ((0, 2),)),
        "pool_bias": noise(splits[8], (4, GROUP_DIM), 0.5, 3.0, ((0, 2),), jnp.float32),
        "pool_gain": jnp.clip(1.0 + 0.18 * jax.random.normal(splits[9], (POOL_WIDTH,), jnp.float32), 0.1, 1.9),
        "ret_gain": jnp.clip(1.0 + 0.18 * jax.random.normal(splits[10], (RET_WIDTH,), jnp.float32), 0.1, 1.9),
        "w_out_pool": noise(splits[11], (POOL_WIDTH, D), (POOL_WIDTH + RET_WIDTH) ** -0.5, 0.125, ((0, 2),)),
        "w_out_ret": noise(splits[12], (RET_WIDTH, D), (POOL_WIDTH + RET_WIDTH) ** -0.5, 0.125, ((0, 2),)),
    }


def rotary(values, positions):
    half = values.shape[-1] // 2
    inverse = 10000.0 ** (-jnp.arange(half, dtype=jnp.float32) / half)
    angles = positions[:, None] * inverse[None, :]
    cosine = jnp.cos(angles)[:, None, :]
    sine = jnp.sin(angles)[:, None, :]
    first = values[..., :half]
    second = values[..., half:]
    return jnp.concatenate([first * cosine - second * sine, second * cosine + first * sine], axis=-1)

def retain(query, key, value, log_decay):
    length = query.shape[0]
    blocks = length // BLOCK
    hp = lax.Precision.HIGHEST

    def split(values):
        return values.reshape(blocks, BLOCK, HEADS, HEAD_DIM).transpose(0, 2, 1, 3)
    steps = jnp.arange(BLOCK, dtype=jnp.float32)
    apart = steps[:, None] - steps[None, :]
    inner = jnp.where(apart[None] >= 0, jnp.exp(log_decay[:, None, None] * jnp.maximum(apart, 0.0)[None]), 0.0)
    query_decay = jnp.exp(log_decay[:, None] * (steps[None, :] + 1.0))
    key_decay = jnp.exp(log_decay[:, None] * (BLOCK - 1.0 - steps[None, :]))
    block_decay = jnp.exp(log_decay * BLOCK)

    def advance(state, pieces):
        qb, kb, vb = pieces
        scores = jnp.einsum('hid,hjd->hij', qb, kb, precision=hp) * inner
        out = jnp.einsum('hij,hje->hie', scores, vb, precision=hp)
        out = out + jnp.einsum('hid,hde->hie', qb, state, precision=hp) * query_decay[:, :, None]
        state = state * block_decay[:, None, None] + jnp.einsum('hjd,hje->hde', kb * key_decay[:, :, None], vb, precision=hp)
        return (state, out)
    start = jnp.zeros((HEADS, HEAD_DIM, HEAD_DIM), jnp.float32)
    state, outs = lax.scan(advance, start, (split(query), split(key), split(value)))
    return outs.transpose(0, 2, 1, 3).reshape(length, HEADS, HEAD_DIM)

def reference(tokens, norm_gain, w_pool, w_query, w_key, w_value, w_gate, pool_mix, pool_bias, pool_gain, ret_gain, w_out_pool, w_out_ret):
    xf = tokens.astype(jnp.float32)
    normed = (xf * lax.rsqrt(lax.optimization_barrier(jnp.mean(xf * xf, axis=-1, keepdims=True)) + 1e-06) * norm_gain).astype(jnp.bfloat16)
    pool_in = jnp.dot(normed, w_pool, preferred_element_type=jnp.float32).astype(jnp.bfloat16)
    query = jnp.dot(normed, w_query, preferred_element_type=jnp.float32).astype(jnp.bfloat16)
    key = jnp.dot(normed, w_key, preferred_element_type=jnp.float32).astype(jnp.bfloat16)
    value = jnp.dot(normed, w_value, preferred_element_type=jnp.float32).astype(jnp.bfloat16)
    gate = jnp.dot(normed, w_gate, preferred_element_type=jnp.float32).astype(jnp.bfloat16)
    positions = jnp.arange(SEQ, dtype=jnp.float32)
    groups = []
    for group in range(4):
        window = 2 ** (group + 1)
        block = pool_in[:, group * GROUP_DIM:(group + 1) * GROUP_DIM].astype(jnp.float32)
        running = jnp.cumsum(block, axis=0)
        padded = jnp.concatenate([jnp.zeros((window, GROUP_DIM), jnp.float32), running], axis=0)
        window_sum = padded[window:] - padded[:SEQ]
        count = jnp.minimum(positions + 1.0, float(window))[:, None]
        diff = (window_sum / count - block).astype(jnp.bfloat16)
        mixed_group = jnp.dot(diff, pool_mix[group], preferred_element_type=jnp.float32) + pool_bias[group][None, :]
        groups.append(mixed_group)
    pool_out = (jnp.concatenate(groups, axis=1) * pool_gain[None, :]).astype(jnp.bfloat16)
    head_ids = jnp.arange(HEADS, dtype=jnp.float32)
    log_decay = -2.0 ** (-5) * (SEQ / 16.0) ** (-2.0 * head_ids / (HEADS - 1))
    qf = rotary(query.astype(jnp.float32).reshape(SEQ, HEADS, HEAD_DIM), positions)
    kf = rotary(key.astype(jnp.float32).reshape(SEQ, HEADS, HEAD_DIM), positions) * HEAD_DIM ** (-0.5)
    vf = value.astype(jnp.float32).reshape(SEQ, HEADS, HEAD_DIM)
    raw = retain(qf, kf, vf, log_decay)
    mean = lax.optimization_barrier(jnp.mean(raw, axis=-1, keepdims=True))
    var = lax.optimization_barrier(jnp.mean(jnp.square(raw - mean), axis=-1, keepdims=True))
    normalized = ((raw - mean) * lax.rsqrt(var + 1e-06)).reshape(SEQ, RET_WIDTH) * ret_gain[None, :]
    ret_out = (jax.nn.silu(gate.astype(jnp.float32)) * normalized).astype(jnp.bfloat16)
    pool_share = POOL_WIDTH // N_TP
    ret_share = RET_WIDTH // N_TP
    total = jnp.zeros((SEQ, D), jnp.float32)
    for index in range(N_TP):
        part_pool = jnp.dot(pool_out[:, index * pool_share:(index + 1) * pool_share], w_out_pool[index * pool_share:(index + 1) * pool_share], preferred_element_type=jnp.float32)
        part_ret = jnp.dot(ret_out[:, index * ret_share:(index + 1) * ret_share], w_out_ret[index * ret_share:(index + 1) * ret_share], preferred_element_type=jnp.float32)
        total = total + (part_pool + part_ret).astype(jnp.bfloat16).astype(jnp.float32)
    return total.astype(jnp.bfloat16)
```

```python
import functools
import math

import jax
import jax.numpy as jnp
from jax import lax
from jax.experimental import pallas as pl
from jax.experimental.pallas import tpu as pltpu
from jax.sharding import PartitionSpec as P

GROUP_DIM = 256
HEAD_DIM = 128
CHUNK = 256
SUB = 128
RIM = 16
HOP = 4
PIECE = 128
STEP = 16
F32 = jnp.float32
BF16 = jnp.bfloat16
MESH = pl.DeviceIdType.MESH


def dot(a, b):
    return jnp.dot(a, b, preferred_element_type=F32)


def layer_kernel(
    n_sp,
    n_tp,
    tokens,
    norm_gain,
    w_pool,
    w_query,
    w_key,
    w_value,
    w_gate,
    pool_mix,
    pool_bias,
    pool_gain,
    ret_gain,
    w_out_pool,
    w_out_ret,
    out_own,
    x_in,
    tok_own,
    tok_oth,
    wts,
    wo,
    ngain,
    pmix,
    pbias,
    pgain,
    rgain,
    pv,
    pp,
    gated,
    kr,
    qr,
    raw,
    pool_out,
    ret,
    cosine,
    sine,
    decay,
    qdec,
    kdec,
    fresh,
    states,
    total,
    sin_buf,
    sout_buf,
    band,
    ldec,
    acc,
    part_send,
    part_recv,
    x_sem,
    w_sem,
    wo_sem,
    small_sem,
    tok_ss,
    tok_rs,
    st_send,
    st_recv,
    rim_rs,
    part_ss,
    part_rs,
):
    tp = lax.axis_index("tp")
    sp = lax.axis_index("sp")
    rows = tokens.shape[0]
    length = rows * n_tp
    width = w_query.shape[1]
    pool_width = w_pool.shape[1]
    wide = wo.shape[1]
    heads = width // HEAD_DIM
    groups = pool_width // GROUP_DIM
    chunks = length // CHUNK
    per_half = rows // CHUNK
    pieces = rows // PIECE
    seq_len = length * n_sp
    own = pl.multiple_of(tp * rows, rows)
    other = pl.multiple_of((n_tp - 1 - tp) * rows, rows)
    peer = {"tp": n_tp - 1 - tp}

    gain_in = pltpu.make_async_copy(norm_gain, ngain, small_sem.at[0])
    gain_in.start()
    x_copies = []
    for i in range(pieces):
        at = pl.ds(i * PIECE, PIECE)
        x_copies.append(pltpu.make_async_copy(tokens.at[at], x_in.at[at], x_sem.at[i]))
        x_copies[i].start()
    w_in = [
        pltpu.make_async_copy(w, wts.at[i], w_sem.at[i])
        for i, w in enumerate((w_key, w_value, w_pool, w_query, w_gate))
    ]
    smalls = [
        pltpu.make_async_copy(src, dst, small_sem.at[i + 1])
        for i, (src, dst) in enumerate(
            ((pool_mix, pmix), (pool_bias, pbias), (pool_gain, pgain), (ret_gain, rgain))
        )
    ]
    wo_in = [
        pltpu.make_async_copy(w_out_pool, wo.at[pl.ds(0, pool_width)], wo_sem.at[0]),
        pltpu.make_async_copy(w_out_ret, wo.at[pl.ds(pool_width, width)], wo_sem.at[1]),
    ]
    for copy in w_in + smalls + wo_in:
        copy.start()

    barrier = pltpu.get_barrier_semaphore()
    pl.semaphore_signal(barrier, inc=1, device_id=peer, device_id_type=MESH)

    @pl.when(sp > 0)
    def _():
        pl.semaphore_signal(barrier, inc=1, device_id={"sp": sp - 1}, device_id_type=MESH)

    @pl.when(sp < n_sp - 1)
    def _():
        pl.semaphore_signal(barrier, inc=1, device_id={"sp": sp + 1}, device_id_type=MESH)

    def log_decay(h):
        total_heads = heads * n_tp
        value = jnp.float32(0.0)
        for t in range(n_tp):
            one = -(2.0**-5) * (seq_len / 16.0) ** (-2.0 * (t * heads + h) / (total_heads - 1))
            value = jnp.where(tp == t, jnp.float32(one), value)
        return value

    logs = [log_decay(h) for h in range(heads)]
    lane = lax.broadcasted_iota(jnp.int32, (SUB, HEAD_DIM), 1)
    row = lax.broadcasted_iota(jnp.int32, (SUB, HEAD_DIM), 0)
    hd = HEAD_DIM // 2
    low = lane < hd
    freq = jnp.exp(
        jnp.where(low, lane, lane - hd).astype(F32) * (-math.log(10000.0) / hd)
    )
    ang = row.astype(F32) * freq
    cos_r, sin_r = jnp.cos(ang), jnp.sin(ang)
    subs = length // SUB
    base_row = lax.broadcasted_iota(jnp.int32, (subs, HEAD_DIM), 0)
    base = (sp * length + base_row * SUB).astype(F32) * freq[:subs]
    cos_b, sin_b = jnp.cos(base), jnp.sin(base)
    for b in range(subs):
        cb, sb = cos_b[b : b + 1], sin_b[b : b + 1]
        cosine[b * SUB : (b + 1) * SUB] = cb * cos_r - sb * sin_r
        s = sb * cos_r + cb * sin_r
        sine[b * SUB : (b + 1) * SUB] = jnp.where(low, -s, s)

    step_i = lax.broadcasted_iota(jnp.int32, (CHUNK, HEAD_DIM), 0).astype(F32)
    di = lax.broadcasted_iota(jnp.int32, (CHUNK, CHUNK), 0) - lax.broadcasted_iota(
        jnp.int32, (CHUNK, CHUNK), 1
    )
    dpos = jnp.maximum(di, 0).astype(F32)
    for h in range(heads):
        decay[h] = jnp.where(di >= 0, jnp.exp(logs[h] * dpos), 0.0)
        qdec[h] = jnp.exp(logs[h] * (step_i + 1.0))
        kdec[h] = jnp.exp(logs[h] * (CHUNK - 1.0 - step_i))
        ldec[h] = jnp.exp(jnp.full((8, HEAD_DIM), logs[h] * length, F32))
    bi = lax.broadcasted_iota(jnp.int32, (SUB, SUB + RIM), 0)
    bj = lax.broadcasted_iota(jnp.int32, (SUB, SUB + RIM), 1)
    back = bi + RIM - bj
    windows = [jnp.left_shift(jnp.int32(2), tp * groups + g) for g in range(groups)]
    for g in range(groups):
        band[g] = jnp.where((back >= 0) & (back < windows[g]), 1.0, 0.0).astype(BF16)

    sin_buf[heads] = jnp.zeros((HEAD_DIM, HEAD_DIM), BF16)

    @pl.when(sp == 0)
    def _():
        pp[0:RIM] = jnp.zeros((RIM, pool_width), BF16)
        sin_buf[...] = jnp.zeros_like(sin_buf)

    def tok_copy(i):
        at = pl.ds(i * PIECE, PIECE)
        return pltpu.make_async_remote_copy(
            src_ref=tok_own.at[at],
            dst_ref=tok_oth.at[at],
            send_sem=tok_ss.at[i],
            recv_sem=tok_rs.at[i],
            device_id=peer,
            device_id_type=MESH,
        )

    def norm_piece(i):
        starts = range(i * PIECE, (i + 1) * PIECE, STEP)
        scales = []
        for r in starts:
            x = x_in[r : r + STEP, :].astype(F32)
            scales.append(lax.rsqrt(jnp.mean(x * x, axis=-1, keepdims=True) + 1e-06))
        for r, scale in zip(starts, scales):
            x = x_in[r : r + STEP, :].astype(F32)
            tok_own[r : r + STEP, :] = (x * scale * ngain[...]).astype(BF16)

    def rotate(x, at):
        return x * cosine[at] + pltpu.roll(x, HEAD_DIM // 2, 1) * sine[at]

    def place(base_pos, j):
        return pl.multiple_of(base_pos + j * CHUNK, CHUNK)

    def project(w, src, j):
        return dot(src[j * CHUNK : (j + 1) * CHUNK, :], wts[w])

    def kv_chunk(src, base_pos, j):
        start = place(base_pos, j)
        at = pl.ds(start, CHUNK)
        key = project(0, src, j)
        kds = []
        for h in range(heads):
            cols = slice(h * HEAD_DIM, (h + 1) * HEAD_DIM)
            k = rotate(key[:, cols].astype(BF16).astype(F32), at) * HEAD_DIM**-0.5
            kr[at, cols] = k.astype(BF16)
            kds.append((k * kdec[h]).astype(BF16))
        value = project(1, src, j).astype(BF16)
        pv[at] = value
        c = start // CHUNK
        for h in range(heads):
            cols = slice(h * HEAD_DIM, (h + 1) * HEAD_DIM)
            fresh[c, h] = lax.dot_general(
                kds[h], value[:, cols], (((0,), (0,)), ((), ())), preferred_element_type=F32
            )

    def pool_chunk(src, base_pos, j):
        at = pl.ds(pl.multiple_of(place(base_pos, j) + RIM, RIM), CHUNK)
        pp[at] = project(2, src, j).astype(BF16)

    def query_chunk(src, base_pos, j):
        at = pl.ds(place(base_pos, j), CHUNK)
        q = project(3, src, j)
        for h in range(heads):
            cols = slice(h * HEAD_DIM, (h + 1) * HEAD_DIM)
            qr[at, cols] = rotate(q[:, cols].astype(BF16).astype(F32), at).astype(BF16)

    def gate_chunk(src, base_pos, j):
        at = pl.ds(place(base_pos, j), CHUNK)
        g = project(4, src, j).astype(BF16).astype(F32)
        gated[at] = g * (1.0 / (1.0 + jnp.exp(-g))) * rgain[...]

    def intra(base_pos, j):
        at = pl.ds(place(base_pos, j), CHUNK)
        for h in range(heads):
            cols = slice(h * HEAD_DIM, (h + 1) * HEAD_DIM)
            scores = lax.dot_general(
                qr[at, cols], kr[at, cols], (((1,), (1,)), ((), ())), preferred_element_type=F32
            )
            raw[at, cols] = dot((scores * decay[h]).astype(BF16), pv[at, cols])

    def pool_mixing(c):
        for s in range(CHUNK // SUB):
            first = c * CHUNK + s * SUB
            here = sp * length + first + lax.broadcasted_iota(jnp.int32, (SUB, GROUP_DIM), 0)
            for g in range(groups):
                cols = slice(g * GROUP_DIM, (g + 1) * GROUP_DIM)
                span = pp[first : first + SUB + RIM, cols]
                x = pp[first + RIM : first + RIM + SUB, cols].astype(F32)
                count = jnp.minimum(here + 1, windows[g]).astype(F32)
                diff = (dot(band[g], span) / count - x).astype(BF16)
                mixed = dot(diff, pmix[g]) + pbias[g : g + 1]
                pool_out[first : first + SUB, cols] = (mixed * pgain[:, cols]).astype(BF16)

    def st_copy(h):
        return pltpu.make_async_remote_copy(
            src_ref=sout_buf.at[h],
            dst_ref=sin_buf.at[h],
            send_sem=st_send.at[h],
            recv_sem=st_recv.at[h],
            device_id={"sp": sp + 1},
            device_id_type=MESH,
        )

    rim_copy = pltpu.make_async_remote_copy(
        src_ref=pp.at[pl.ds(length, RIM)],
        dst_ref=pp.at[pl.ds(0, RIM)],
        send_sem=rim_rs.at[0],
        recv_sem=rim_rs.at[1],
        device_id={"sp": sp + 1},
        device_id_type=MESH,
    )

    def pass_on(slot, h):
        sout_buf[slot] = (total[h] + ldec[h, 0:1] * sin_buf[slot].astype(F32)).astype(BF16)

    def relay(c):
        h = c - HOP * (sp - 1)
        active = (h >= 0) & (h < heads) & (sp > 0) & (sp < n_sp - 1)
        slot = jnp.where(active, h, heads)

        @pl.when(active)
        def _():
            st_copy(h).wait_recv()

        pass_on(slot, jnp.where(active, h, 0))

        @pl.when(active)
        def _():
            st_copy(h).start()

    slots = 8

    x_copies[0].wait()
    x_copies[1].wait()
    gain_in.wait()
    norm_piece(0)
    neighbours = jnp.where(sp > 0, 1, 0) + jnp.where(sp < n_sp - 1, 1, 0)
    pl.semaphore_wait(barrier, 1 + neighbours)
    tok_copy(0).start()
    norm_piece(1)
    tok_copy(1).start()
    for i in range(2, pieces):
        x_copies[i].wait()
    w_in[0].wait()
    w_in[1].wait()
    kv_chunk(tok_own, own, 0)
    for i in range(2, pieces):
        norm_piece(i)
    for i in range(2, pieces):
        tok_copy(i).start()
    w_in[2].wait()
    for j in range(1, per_half):
        kv_chunk(tok_own, own, j)
    pool_chunk(tok_own, own, 0)
    for i in range(pieces):
        tok_copy(i).wait_recv()
    for j in range(per_half):
        kv_chunk(tok_oth, other, j)

    for h in range(heads):
        step = jnp.exp(jnp.full((1, HEAD_DIM), logs[h] * CHUNK, F32))
        run = fresh[0, h]
        states[0, h] = jnp.zeros((HEAD_DIM, HEAD_DIM), F32)
        for c in range(1, chunks):
            states[c, h] = run
            run = run * step + fresh[c, h]
        total[h] = run
        sout_buf[h] = run.astype(BF16)

    @pl.when((sp == 0) & (sp < n_sp - 1))
    def _():
        for h in range(heads):
            st_copy(h).start()

    w_in[3].wait()
    for j in range(1, per_half):
        pool_chunk(tok_own, own, j)
    for j in range(per_half):
        pool_chunk(tok_oth, other, j)

    @pl.when(sp < n_sp - 1)
    def _():
        rim_copy.start()

    for copy in w_in[4:] + smalls:
        copy.wait()

    query_chunk(tok_own, own, 0)
    query_chunk(tok_own, own, 1)
    relay(0)
    query_chunk(tok_oth, other, 0)
    relay(1)
    query_chunk(tok_oth, other, 1)
    relay(2)
    gate_chunk(tok_own, own, 0)
    intra(own, 0)
    pool_mixing(1)
    relay(3)
    gate_chunk(tok_own, own, 1)
    intra(own, 1)
    pool_mixing(2)
    relay(4)
    gate_chunk(tok_oth, other, 0)
    intra(other, 0)
    pool_mixing(3)
    relay(5)

    @pl.when(sp > 0)
    def _():
        rim_copy.wait_recv()

    gate_chunk(tok_oth, other, 1)
    intra(other, 1)
    pool_mixing(0)
    for copy in wo_in:
        copy.wait()
    relay(6)

    tile = 512

    def pool_share(base_pos, j):
        at = pl.ds(place(base_pos, j), CHUNK)
        mine = slice(j * CHUNK, (j + 1) * CHUNK)
        for n in range(wide // tile):
            cols = slice(n * tile, (n + 1) * tile)
            acc[mine, cols] = dot(pool_out[at, :], wo[:pool_width, cols])

    pool_share(other, 0)
    relay(7)
    pool_share(other, 1)

    def rest(h, carry):
        late = (h + HOP * (sp - 1) >= slots) | (sp == n_sp - 1)

        @pl.when(late & (sp > 0))
        def _():
            st_copy(h).wait_recv()

            @pl.when(sp < n_sp - 1)
            def _():
                pass_on(h, h)
                st_copy(h).start()

        return carry

    lax.fori_loop(0, heads, rest, 0)

    def finish(base_pos, j):
        start = place(base_pos, j)
        at = pl.ds(start, CHUNK)
        c = start // CHUNK
        for h in range(heads):
            cols = slice(h * HEAD_DIM, (h + 1) * HEAD_DIM)
            ahead = jnp.exp(jnp.full((1, HEAD_DIM), logs[h], F32) * start.astype(F32))
            state = (states[c, h] + sin_buf[h].astype(F32) * ahead).astype(BF16)
            r = raw[at, cols] + qdec[h] * dot(qr[at, cols], state)
            r = r - jnp.mean(r, axis=-1, keepdims=True)
            var = jnp.mean(r * r, axis=-1, keepdims=True)
            ret[at, cols] = (gated[at, cols] * (r * lax.rsqrt(var + 1e-06))).astype(BF16)

    def part_copy(j):
        at = pl.ds(j * CHUNK, CHUNK)
        return pltpu.make_async_remote_copy(
            src_ref=part_send.at[at],
            dst_ref=part_recv.at[at],
            send_sem=part_ss.at[j],
            recv_sem=part_rs.at[j],
            device_id=peer,
            device_id_type=MESH,
        )

    def multiply_other(j):
        at = pl.ds(place(other, j), CHUNK)
        mine = slice(j * CHUNK, (j + 1) * CHUNK)
        for n in range(wide // tile):
            cols = slice(n * tile, (n + 1) * tile)
            part_send[mine, cols] = (
                acc[mine, cols] + dot(ret[at, :], wo[pool_width:, cols])
            ).astype(BF16)

    def multiply_own(j):
        at = pl.ds(place(own, j), CHUNK)
        mine = slice(j * CHUNK, (j + 1) * CHUNK)
        left = jnp.concatenate([pool_out[at, :], ret[at, :]], axis=1)
        for n in range(wide // tile):
            cols = slice(n * tile, (n + 1) * tile)
            out_own[mine, cols] = dot(left, wo[:, cols]).astype(BF16)

    def add_received(j):
        mine = slice(j * CHUNK, (j + 1) * CHUNK)
        out_own[mine] = (out_own[mine].astype(F32) + part_recv[mine].astype(F32)).astype(BF16)

    finish(other, 0)
    for j in range(per_half):
        multiply_other(j)
        if j + 1 < per_half:
            finish(other, j + 1)
        else:
            finish(own, 0)
        part_copy(j).start()
    for j in range(per_half):
        multiply_own(j)
        if j > 0:
            add_received(j - 1)
        if j + 1 < per_half:
            finish(own, j + 1)
        part_copy(j).wait_recv()
    add_received(per_half - 1)

    for i in range(pieces):
        tok_copy(i).wait_send()
    for j in range(per_half):
        part_copy(j).wait_send()

    @pl.when(sp < n_sp - 1)
    def _():
        rim_copy.wait_send()
        for h in range(heads):
            st_copy(h).wait_send()


def per_device(
    tokens,
    norm_gain,
    w_pool,
    w_query,
    w_key,
    w_value,
    w_gate,
    pool_mix,
    pool_bias,
    pool_gain,
    ret_gain,
    w_out_pool,
    w_out_ret,
):
    n_sp, n_tp = lax.axis_size("sp"), lax.axis_size("tp")
    rows, model = tokens.shape
    length = rows * n_tp
    width = w_query.shape[1]
    heads = width // HEAD_DIM
    pool_width = w_pool.shape[1]
    groups = pool_width // GROUP_DIM
    chunks = length // CHUNK
    per_half = rows // CHUNK
    pieces = rows // PIECE
    wide = w_out_pool.shape[1]
    hbm = pl.BlockSpec(memory_space=pltpu.HBM)
    vmem = pl.BlockSpec(memory_space=pltpu.VMEM)
    dma = pltpu.SemaphoreType.DMA
    flops = 2 * length * model * (pool_width + 4 * width) + 2 * length * (pool_width + width) * wide
    return pl.pallas_call(
        functools.partial(layer_kernel, n_sp, n_tp),
        out_shape=pltpu.VMEM((rows, wide), BF16),
        in_specs=[hbm] * 13,
        out_specs=vmem,
        scratch_shapes=[
            pltpu.VMEM((rows, model), BF16),
            pltpu.VMEM((rows, model), BF16),
            pltpu.VMEM((rows, model), BF16),
            pltpu.VMEM((5, model, width), BF16),
            pltpu.VMEM((pool_width + width, wide), BF16),
            pltpu.VMEM((1, model), F32),
            pltpu.VMEM((groups, GROUP_DIM, GROUP_DIM), BF16),
            pltpu.VMEM((groups, GROUP_DIM), F32),
            pltpu.VMEM((1, pool_width), F32),
            pltpu.VMEM((1, width), F32),
            pltpu.VMEM((length, width), BF16),
            pltpu.VMEM((length + RIM, pool_width), BF16),
            pltpu.VMEM((length, width), F32),
            pltpu.VMEM((length, width), BF16),
            pltpu.VMEM((length, width), BF16),
            pltpu.VMEM((length, width), F32),
            pltpu.VMEM((length, pool_width), BF16),
            pltpu.VMEM((length, width), BF16),
            pltpu.VMEM((length, HEAD_DIM), F32),
            pltpu.VMEM((length, HEAD_DIM), F32),
            pltpu.VMEM((heads, CHUNK, CHUNK), F32),
            pltpu.VMEM((heads, CHUNK, HEAD_DIM), F32),
            pltpu.VMEM((heads, CHUNK, HEAD_DIM), F32),
            pltpu.VMEM((chunks, heads, HEAD_DIM, HEAD_DIM), F32),
            pltpu.VMEM((chunks, heads, HEAD_DIM, HEAD_DIM), F32),
            pltpu.VMEM((heads, HEAD_DIM, HEAD_DIM), F32),
            pltpu.VMEM((heads + 1, HEAD_DIM, HEAD_DIM), BF16),
            pltpu.VMEM((heads + 1, HEAD_DIM, HEAD_DIM), BF16),
            pltpu.VMEM((groups, SUB, SUB + RIM), BF16),
            pltpu.VMEM((heads, 8, HEAD_DIM), F32),
            pltpu.VMEM((rows, wide), F32),
            pltpu.VMEM((rows, wide), BF16),
            pltpu.VMEM((rows, wide), BF16),
            dma((pieces,)),
            dma((5,)),
            dma((2,)),
            dma((5,)),
            dma((pieces,)),
            dma((pieces,)),
            dma((heads,)),
            dma((heads,)),
            dma((2,)),
            dma((per_half,)),
            dma((per_half,)),
        ],
        compiler_params=pltpu.CompilerParams(
            collective_id=0, has_side_effects=True, vmem_limit_bytes=56 * 1024 * 1024
        ),
        cost_estimate=pl.CostEstimate(
            flops=flops, bytes_accessed=20 * 1024 * 1024, transcendentals=0
        ),
    )(
        tokens,
        norm_gain.reshape(1, -1),
        w_pool,
        w_query,
        w_key,
        w_value,
        w_gate,
        pool_mix,
        pool_bias,
        pool_gain.reshape(1, -1),
        ret_gain.reshape(1, -1),
        w_out_pool,
        w_out_ret,
    )


def solution(mesh):
    return jax.shard_map(
        per_device,
        mesh=mesh,
        in_specs=(
            P(("fs", "sp", "tp"), None),
            P(),
            P(None, "tp"),
            P(None, "tp"),
            P(None, "tp"),
            P(None, "tp"),
            P(None, "tp"),
            P("tp", None, None),
            P("tp", None),
            P("tp"),
            P("tp"),
            P("tp", None),
            P("tp", None),
        ),
        out_specs=P(("fs", "sp", "tp"), None),
        check_vma=False,
    )
```

```python
import functools
import math

import jax
import jax.numpy as jnp
from jax import lax
from jax.experimental import pallas as pl
from jax.experimental.pallas import tpu as pltpu
from jax.sharding import PartitionSpec as P

GROUP_DIM = 256
HEAD_DIM = 128
CHUNK = 256
SUB = 128
RIM = 16
HOP = 4
PIECE = 128
STEP = 16
TILE = 512
F32 = jnp.float32
BF16 = jnp.bfloat16
MESH = pl.DeviceIdType.MESH


def dot(a, b):
    return jnp.dot(a, b, preferred_element_type=F32)


def layer_kernel(
    n_sp,
    n_tp,
    tokens,
    norm_gain,
    w_pool,
    w_query,
    w_key,
    w_value,
    w_gate,
    pool_mix,
    pool_bias,
    pool_gain,
    ret_gain,
    w_out_pool,
    w_out_ret,
    out_own,
    x_in,
    tok_own,
    tok_oth,
    wts,
    wo,
    ngain,
    pmix,
    pbias,
    pgain,
    rgain,
    pv,
    pp,
    gated,
    kr,
    kd,
    qr,
    weights,
    raw,
    pool_diff,
    pool_out,
    ret,
    cosine,
    sine,
    decay,
    qdec,
    kdec,
    fresh,
    states,
    total,
    sin_buf,
    sout_buf,
    band,
    ldec,
    acc,
    part_send,
    part_recv,
    x_sem,
    w_sem,
    wo_sem,
    small_sem,
    tok_ss,
    tok_rs,
    st_send,
    st_recv,
    rim_rs,
    part_ss,
    part_rs,
):
    tp = lax.axis_index("tp")
    sp = lax.axis_index("sp")
    rows = tokens.shape[0]
    length = rows * n_tp
    width = w_query.shape[1]
    pool_width = w_pool.shape[1]
    wide = w_out_pool.shape[1]
    tiles = wide // TILE
    blocks = tokens.shape[1] // TILE
    heads = width // HEAD_DIM
    groups = pool_width // GROUP_DIM
    chunks = length // CHUNK
    per_half = rows // CHUNK
    pieces = rows // PIECE
    seq_len = length * n_sp
    own = pl.multiple_of(tp * rows, rows)
    other = pl.multiple_of((n_tp - 1 - tp) * rows, rows)
    peer = {"tp": n_tp - 1 - tp}

    gain_in = pltpu.make_async_copy(norm_gain, ngain, small_sem.at[0])
    gain_in.start()
    x_copies = []
    for i in range(pieces):
        at = pl.ds(i * PIECE, PIECE)
        x_copies.append(pltpu.make_async_copy(tokens.at[at], x_in.at[at], x_sem.at[i]))
        x_copies[i].start()
    w_in = [
        pltpu.make_async_copy(w, wts.at[i], w_sem.at[i])
        for i, w in enumerate((w_key, w_value, w_pool, w_query, w_gate))
    ]
    smalls = [
        pltpu.make_async_copy(src, dst, small_sem.at[i + 1])
        for i, (src, dst) in enumerate(
            ((pool_mix, pmix), (pool_bias, pbias), (pool_gain, pgain), (ret_gain, rgain))
        )
    ]
    wo_in = [
        pltpu.make_async_copy(
            src.at[:, pl.ds(n * TILE, TILE)],
            wo.at[n, pl.ds(low, src.shape[0])],
            wo_sem.at[i, n],
        )
        for i, (src, low) in enumerate(((w_out_pool, 0), (w_out_ret, pool_width)))
        for n in range(tiles)
    ]
    w_in[0].start()
    for copy in w_in[1:]:
        copy.start(priority=1)

    barrier = pltpu.get_barrier_semaphore()
    pl.semaphore_signal(barrier, inc=1, device_id=peer, device_id_type=MESH)

    @pl.when(sp > 0)
    def _():
        pl.semaphore_signal(barrier, inc=1, device_id={"sp": sp - 1}, device_id_type=MESH)

    @pl.when(sp < n_sp - 1)
    def _():
        pl.semaphore_signal(barrier, inc=1, device_id={"sp": sp + 1}, device_id_type=MESH)

    def log_decay(h):
        total_heads = heads * n_tp
        value = jnp.float32(0.0)
        for t in range(n_tp):
            one = -(2.0**-5) * (seq_len / 16.0) ** (-2.0 * (t * heads + h) / (total_heads - 1))
            value = jnp.where(tp == t, jnp.float32(one), value)
        return value

    logs = [log_decay(h) for h in range(heads)]
    lane = lax.broadcasted_iota(jnp.int32, (SUB, HEAD_DIM), 1)
    row = lax.broadcasted_iota(jnp.int32, (SUB, HEAD_DIM), 0)
    hd = HEAD_DIM // 2
    low = lane < hd
    freq = jnp.exp(
        jnp.where(low, lane, lane - hd).astype(F32) * (-math.log(10000.0) / hd)
    )
    ang = row.astype(F32) * freq
    cos_r, sin_r = jnp.cos(ang), jnp.sin(ang)
    subs = length // SUB
    base_row = lax.broadcasted_iota(jnp.int32, (subs, HEAD_DIM), 0)
    base = (sp * length + base_row * SUB).astype(F32) * freq[:subs]
    cos_b, sin_b = jnp.cos(base), jnp.sin(base)
    for b in range(subs):
        cb, sb = cos_b[b : b + 1], sin_b[b : b + 1]
        cosine[b * SUB : (b + 1) * SUB] = cb * cos_r - sb * sin_r
        s = sb * cos_r + cb * sin_r
        sine[b * SUB : (b + 1) * SUB] = jnp.where(low, -s, s)

    step_i = lax.broadcasted_iota(jnp.int32, (CHUNK, HEAD_DIM), 0).astype(F32)
    di = lax.broadcasted_iota(jnp.int32, (CHUNK, CHUNK), 0) - lax.broadcasted_iota(
        jnp.int32, (CHUNK, CHUNK), 1
    )
    dpos = jnp.maximum(di, 0).astype(F32)
    for h in range(heads):
        decay[h] = jnp.where(di >= 0, jnp.exp(logs[h] * dpos), 0.0)
        qdec[h] = jnp.exp(logs[h] * (step_i + 1.0))
        kdec[h] = jnp.exp(logs[h] * (CHUNK - 1.0 - step_i))
        ldec[h] = jnp.exp(jnp.full((8, HEAD_DIM), logs[h] * length, F32))
    bi = lax.broadcasted_iota(jnp.int32, (SUB, SUB + RIM), 0)
    bj = lax.broadcasted_iota(jnp.int32, (SUB, SUB + RIM), 1)
    back = bi + RIM - bj
    windows = [jnp.left_shift(jnp.int32(2), tp * groups + g) for g in range(groups)]
    for g in range(groups):
        band[g] = jnp.where((back >= 0) & (back < windows[g]), 1.0, 0.0).astype(BF16)

    sin_buf[heads] = jnp.zeros((HEAD_DIM, HEAD_DIM), BF16)

    @pl.when(sp == 0)
    def _():
        pp[0:RIM] = jnp.zeros((RIM, pool_width), BF16)
        sin_buf[...] = jnp.zeros_like(sin_buf)

    def tok_copy(i):
        at = pl.ds(i * PIECE, PIECE)
        return pltpu.make_async_remote_copy(
            src_ref=tok_own.at[:, at],
            dst_ref=tok_oth.at[:, at],
            send_sem=tok_ss.at[i],
            recv_sem=tok_rs.at[i],
            device_id=peer,
            device_id_type=MESH,
        )

    def norm_piece(i):
        starts = range(i * PIECE, (i + 1) * PIECE, STEP)
        scales = []
        for r in starts:
            x = x_in[r : r + STEP, :].astype(F32)
            scales.append(lax.rsqrt(jnp.mean(x * x, axis=-1, keepdims=True) + 1e-06))
        for r, scale in zip(starts, scales):
            x = x_in[r : r + STEP, :].astype(F32)
            normed = (x * scale * ngain[...]).astype(BF16)
            for n in range(blocks):
                tok_own[n, r : r + STEP, :] = normed[:, n * TILE : (n + 1) * TILE]

    def rotate(x, at):
        return x * cosine[at] + pltpu.roll(x, HEAD_DIM // 2, 1) * sine[at]

    half = blocks // 2
    own_at = [(tok_own, own, j) for j in range(per_half)]
    oth_at = [(tok_oth, other, j) for j in range(per_half)]

    def position(unit):
        return pl.multiple_of(unit[1] + unit[2] * CHUNK, CHUNK)

    def project(w, unit, lo=0, hi=blocks, res=None):
        src, _, j = unit
        mine = slice(j * CHUNK, (j + 1) * CHUNK)
        for n in range(lo, hi):
            term = dot(src[n, mine, :], wts[w, n * TILE : (n + 1) * TILE, :])
            res = term if res is None else res + term
        return res

    def split(w, unit, between):
        res = project(w, unit, 0, half)
        between()
        return project(w, unit, half, blocks, res)

    def nothing():
        pass

    def head_cols(h):
        return slice(h * HEAD_DIM, (h + 1) * HEAD_DIM)

    def key_unit(unit, between=nothing):
        at = pl.ds(position(unit), CHUNK)
        key = split(0, unit, between)
        for h in range(heads):
            k = rotate(key[:, head_cols(h)].astype(BF16).astype(F32), at) * HEAD_DIM**-0.5
            kr[at, head_cols(h)] = k.astype(BF16)
            kd[at, head_cols(h)] = (k * kdec[h]).astype(BF16)

    def value_unit(unit, between=nothing):
        pv[pl.ds(position(unit), CHUNK)] = split(1, unit, between).astype(BF16)

    def state_unit(unit):
        start = position(unit)
        at = pl.ds(start, CHUNK)
        for h in range(heads):
            fresh[start // CHUNK, h] = lax.dot_general(
                kd[at, head_cols(h)],
                pv[at, head_cols(h)],
                (((0,), (0,)), ((), ())),
                preferred_element_type=F32,
            )

    def pool_unit(unit, between=nothing):
        at = pl.ds(pl.multiple_of(position(unit) + RIM, RIM), CHUNK)
        pp[at] = split(2, unit, between).astype(BF16)

    def query_unit(unit, between=nothing):
        at = pl.ds(position(unit), CHUNK)
        q = split(3, unit, between)
        for h in range(heads):
            qr[at, head_cols(h)] = rotate(q[:, head_cols(h)].astype(BF16).astype(F32), at).astype(BF16)

    def gate_unit(unit, between=nothing):
        at = pl.ds(position(unit), CHUNK)
        g = split(4, unit, between).astype(BF16).astype(F32)
        gated[at] = g * (1.0 / (1.0 + jnp.exp(-g))) * rgain[...]

    def score_unit(unit):
        at = pl.ds(position(unit), CHUNK)
        for h in range(heads):
            scores = lax.dot_general(
                qr[at, head_cols(h)],
                kr[at, head_cols(h)],
                (((1,), (1,)), ((), ())),
                preferred_element_type=F32,
            )
            weights[h] = (scores * decay[h]).astype(BF16)

    def intra_unit(unit):
        at = pl.ds(position(unit), CHUNK)
        for h in range(heads):
            raw[at, head_cols(h)] = dot(weights[h], pv[at, head_cols(h)])

    def pool_pieces(c):
        for i in range(CHUNK // SUB):
            for g in range(groups):
                yield c * CHUNK + i * SUB, g, slice(g * GROUP_DIM, (g + 1) * GROUP_DIM)

    def pool_windows(c):
        for first, g, cols in pool_pieces(c):
            here = sp * length + first + lax.broadcasted_iota(jnp.int32, (SUB, GROUP_DIM), 0)
            span = pp[first : first + SUB + RIM, cols]
            x = pp[first + RIM : first + RIM + SUB, cols].astype(F32)
            count = jnp.minimum(here + 1, windows[g]).astype(F32)
            pool_diff[first : first + SUB, cols] = (dot(band[g], span) / count - x).astype(BF16)

    def pool_mixing(c):
        for first, g, cols in pool_pieces(c):
            mixed = dot(pool_diff[first : first + SUB, cols], pmix[g]) + pbias[g : g + 1]
            pool_out[first : first + SUB, cols] = (mixed * pgain[:, cols]).astype(BF16)

    def st_copy(h):
        return pltpu.make_async_remote_copy(
            src_ref=sout_buf.at[h],
            dst_ref=sin_buf.at[h],
            send_sem=st_send.at[h],
            recv_sem=st_recv.at[h],
            device_id={"sp": sp + 1},
            device_id_type=MESH,
        )

    rim_copy = pltpu.make_async_remote_copy(
        src_ref=pp.at[pl.ds(length, RIM)],
        dst_ref=pp.at[pl.ds(0, RIM)],
        send_sem=rim_rs.at[0],
        recv_sem=rim_rs.at[1],
        device_id={"sp": sp + 1},
        device_id_type=MESH,
    )

    def pass_on(slot, h):
        sout_buf[slot] = (total[h] + ldec[h, 0:1] * sin_buf[slot].astype(F32)).astype(BF16)

    def relay(c):
        h = c - HOP * (sp - 1)
        active = (h >= 0) & (h < heads) & (sp > 0) & (sp < n_sp - 1)
        slot = jnp.where(active, h, heads)

        @pl.when(active)
        def _():
            st_copy(h).wait_recv()

        pass_on(slot, jnp.where(active, h, 0))

        @pl.when(active)
        def _():
            st_copy(h).start()

    slots = 8

    gain_in.wait()
    x_copies[0].wait()
    norm_piece(0)
    neighbours = jnp.where(sp > 0, 1, 0) + jnp.where(sp < n_sp - 1, 1, 0)
    pl.semaphore_wait(barrier, 1 + neighbours)
    tok_copy(0).start()
    for i in range(1, pieces):
        x_copies[i].wait()
        norm_piece(i)
        tok_copy(i).start()
    w_in[0].wait()
    w_in[1].wait()
    for copy in smalls + wo_in:
        copy.start(priority=1)
    for copy in w_in[2:4]:
        copy.wait()
    per_chunk = CHUNK // PIECE

    def arrive(j):
        def wait():
            for i in range(j * per_chunk, (j + 1) * per_chunk):
                tok_copy(i).wait_recv()

        return wait

    units = own_at + oth_at
    before = None
    for i, unit in enumerate(units):
        key_unit(unit, functools.partial(state_unit, before) if i > 0 else nothing)
        nxt = i + 1 - per_half
        value_unit(unit, arrive(nxt) if 0 <= nxt < per_half else nothing)
        before = unit

    def combine():
        state_unit(before)
        for h in range(heads):
            step = jnp.exp(jnp.full((1, HEAD_DIM), logs[h] * CHUNK, F32))
            run = fresh[0, h]
            states[0, h] = jnp.zeros((HEAD_DIM, HEAD_DIM), F32)
            for c in range(1, chunks):
                states[c, h] = run
                run = run * step + fresh[c, h]
            total[h] = run
            sout_buf[h] = run.astype(BF16)

    pool_unit(units[0], combine)

    @pl.when((sp == 0) & (sp < n_sp - 1))
    def _():
        for h in range(heads):
            st_copy(h).start()

    for unit in units[1:]:
        pool_unit(unit)

    def send_rim():
        @pl.when(sp < n_sp - 1)
        def _():
            rim_copy.start()

    for copy in w_in[4:] + smalls:
        copy.wait()

    query_unit(units[0], send_rim)
    query_unit(units[1])
    query_unit(units[2], functools.partial(relay, 0))
    query_unit(units[3], functools.partial(relay, 1))

    def mid(unit, c, fence):
        def run():
            fence()
            intra_unit(unit)
            pool_windows(c)

        return run

    def relays(*cs):
        def run():
            for c in cs:
                relay(c)

        return run

    def rim_wait():
        relay(6)
        relay(7)

        @pl.when(sp > 0)
        def _():
            rim_copy.wait_recv()

    fences = [relays(2), relays(3, 4), relays(5), rim_wait]
    for i, unit in enumerate(units):
        c = (i + 1) % chunks
        score_unit(unit)
        gate_unit(unit, mid(unit, c, fences[i]))
        pool_mixing(c)
    for copy in wo_in:
        copy.wait()

    def pool_share(j):
        at = pl.ds(position(oth_at[j]), CHUNK)
        mine = slice(j * CHUNK, (j + 1) * CHUNK)
        for n in range(tiles):
            cols = slice(n * TILE, (n + 1) * TILE)
            acc[mine, cols] = dot(pool_out[at, :], wo[n, :pool_width, :])

    for j in range(per_half - 1):
        pool_share(j)
    def rest(h, carry):
        late = (h + HOP * (sp - 1) >= slots) | (sp == n_sp - 1)

        @pl.when(late & (sp > 0))
        def _():
            st_copy(h).wait_recv()

            @pl.when(sp < n_sp - 1)
            def _():
                pass_on(h, h)
                st_copy(h).start()

        return carry

    lax.fori_loop(0, heads, rest, 0)

    def finish(unit):
        start = position(unit)
        at = pl.ds(start, CHUNK)
        c = start // CHUNK
        for h in range(heads):
            cols = head_cols(h)
            ahead = jnp.exp(jnp.full((1, HEAD_DIM), logs[h], F32) * start.astype(F32))
            state = (states[c, h] + sin_buf[h].astype(F32) * ahead).astype(BF16)
            r = raw[at, cols] + qdec[h] * dot(qr[at, cols], state)
            r = r - jnp.mean(r, axis=-1, keepdims=True)
            var = jnp.mean(r * r, axis=-1, keepdims=True)
            ret[at, cols] = (gated[at, cols] * (r * lax.rsqrt(var + 1e-06))).astype(BF16)

    def part_copy(j):
        at = pl.ds(j * CHUNK, CHUNK)
        return pltpu.make_async_remote_copy(
            src_ref=part_send.at[at],
            dst_ref=part_recv.at[at],
            send_sem=part_ss.at[j],
            recv_sem=part_rs.at[j],
            device_id=peer,
            device_id_type=MESH,
        )

    def multiply_other(j, n):
        at = pl.ds(position(oth_at[j]), CHUNK)
        mine = slice(j * CHUNK, (j + 1) * CHUNK)
        cols = slice(n * TILE, (n + 1) * TILE)
        part_send[mine, cols] = (
            acc[mine, cols] + dot(ret[at, :], wo[n, pool_width:, :])
        ).astype(BF16)

    def multiply_own(j, n):
        at = pl.ds(position(own_at[j]), CHUNK)
        mine = slice(j * CHUNK, (j + 1) * CHUNK)
        cols = slice(n * TILE, (n + 1) * TILE)
        out_own[mine, cols] = (
            dot(pool_out[at, :], wo[n, :pool_width, :]) + dot(ret[at, :], wo[n, pool_width:, :])
        ).astype(BF16)

    def add_received(j):
        mine = slice(j * CHUNK, (j + 1) * CHUNK)
        out_own[mine] = (out_own[mine].astype(F32) + part_recv[mine].astype(F32)).astype(BF16)

    order = oth_at + own_at
    finish(order[0])
    pool_share(per_half - 1)
    for i in range(len(order)):
        sending = i < per_half
        for n in range(tiles):
            if n == 1 and 0 < i <= per_half:
                part_copy(i - 1).start()
            if n == 1 and i > per_half:
                part_copy(i - 1 - per_half).wait_recv()
                add_received(i - 1 - per_half)
            if n == 2 and i + 1 < len(order):
                finish(order[i + 1])
            if sending:
                multiply_other(i, n)
            else:
                multiply_own(i - per_half, n)
    part_copy(per_half - 1).wait_recv()
    add_received(per_half - 1)

    for i in range(pieces):
        tok_copy(i).wait_send()
    for j in range(per_half):
        part_copy(j).wait_send()

    @pl.when(sp < n_sp - 1)
    def _():
        rim_copy.wait_send()
        for h in range(heads):
            st_copy(h).wait_send()


def per_device(
    tokens,
    norm_gain,
    w_pool,
    w_query,
    w_key,
    w_value,
    w_gate,
    pool_mix,
    pool_bias,
    pool_gain,
    ret_gain,
    w_out_pool,
    w_out_ret,
):
    n_sp, n_tp = lax.axis_size("sp"), lax.axis_size("tp")
    rows, model = tokens.shape
    length = rows * n_tp
    width = w_query.shape[1]
    heads = width // HEAD_DIM
    pool_width = w_pool.shape[1]
    groups = pool_width // GROUP_DIM
    chunks = length // CHUNK
    per_half = rows // CHUNK
    pieces = rows // PIECE
    wide = w_out_pool.shape[1]
    hbm = pl.BlockSpec(memory_space=pltpu.HBM)
    vmem = pl.BlockSpec(memory_space=pltpu.VMEM)
    dma = pltpu.SemaphoreType.DMA
    flops = 2 * length * model * (pool_width + 4 * width) + 2 * length * (pool_width + width) * wide
    return pl.pallas_call(
        functools.partial(layer_kernel, n_sp, n_tp),
        out_shape=pltpu.VMEM((rows, wide), BF16),
        in_specs=[hbm] * 13,
        out_specs=vmem,
        scratch_shapes=[
            pltpu.VMEM((rows, model), BF16),
            pltpu.VMEM((model // TILE, rows, TILE), BF16),
            pltpu.VMEM((model // TILE, rows, TILE), BF16),
            pltpu.VMEM((5, model, width), BF16),
            pltpu.VMEM((wide // TILE, pool_width + width, TILE), BF16),
            pltpu.VMEM((1, model), F32),
            pltpu.VMEM((groups, GROUP_DIM, GROUP_DIM), BF16),
            pltpu.VMEM((groups, GROUP_DIM), F32),
            pltpu.VMEM((1, pool_width), F32),
            pltpu.VMEM((1, width), F32),
            pltpu.VMEM((length, width), BF16),
            pltpu.VMEM((length + RIM, pool_width), BF16),
            pltpu.VMEM((length, width), F32),
            pltpu.VMEM((length, width), BF16),
            pltpu.VMEM((length, width), BF16),
            pltpu.VMEM((length, width), BF16),
            pltpu.VMEM((heads, CHUNK, CHUNK), BF16),
            pltpu.VMEM((length, width), F32),
            pltpu.VMEM((length, pool_width), BF16),
            pltpu.VMEM((length, pool_width), BF16),
            pltpu.VMEM((length, width), BF16),
            pltpu.VMEM((length, HEAD_DIM), F32),
            pltpu.VMEM((length, HEAD_DIM), F32),
            pltpu.VMEM((heads, CHUNK, CHUNK), F32),
            pltpu.VMEM((heads, CHUNK, HEAD_DIM), F32),
            pltpu.VMEM((heads, CHUNK, HEAD_DIM), F32),
            pltpu.VMEM((chunks, heads, HEAD_DIM, HEAD_DIM), F32),
            pltpu.VMEM((chunks, heads, HEAD_DIM, HEAD_DIM), F32),
            pltpu.VMEM((heads, HEAD_DIM, HEAD_DIM), F32),
            pltpu.VMEM((heads + 1, HEAD_DIM, HEAD_DIM), BF16),
            pltpu.VMEM((heads + 1, HEAD_DIM, HEAD_DIM), BF16),
            pltpu.VMEM((groups, SUB, SUB + RIM), BF16),
            pltpu.VMEM((heads, 8, HEAD_DIM), F32),
            pltpu.VMEM((rows, wide), F32),
            pltpu.VMEM((rows, wide), BF16),
            pltpu.VMEM((rows, wide), BF16),
            dma((pieces,)),
            dma((5,)),
            dma((2, wide // TILE)),
            dma((5,)),
            dma((pieces,)),
            dma((pieces,)),
            dma((heads,)),
            dma((heads,)),
            dma((2,)),
            dma((per_half,)),
            dma((per_half,)),
        ],
        compiler_params=pltpu.CompilerParams(
            collective_id=0, has_side_effects=True, vmem_limit_bytes=56 * 1024 * 1024
        ),
        cost_estimate=pl.CostEstimate(
            flops=flops, bytes_accessed=20 * 1024 * 1024, transcendentals=0
        ),
    )(
        tokens,
        norm_gain.reshape(1, -1),
        w_pool,
        w_query,
        w_key,
        w_value,
        w_gate,
        pool_mix,
        pool_bias,
        pool_gain.reshape(1, -1),
        ret_gain.reshape(1, -1),
        w_out_pool,
        w_out_ret,
    )


def solution(mesh):
    return jax.shard_map(
        per_device,
        mesh=mesh,
        in_specs=(
            P(("fs", "sp", "tp"), None),
            P(),
            P(None, "tp"),
            P(None, "tp"),
            P(None, "tp"),
            P(None, "tp"),
            P(None, "tp"),
            P("tp", None, None),
            P("tp", None),
            P("tp"),
            P("tp"),
            P("tp", None),
            P("tp", None),
        ),
        out_specs=P(("fs", "sp", "tp"), None),
        check_vma=False,
    )
```

```python
import functools
import math

import jax
import jax.numpy as jnp
from jax import lax
from jax.experimental import pallas as pl
from jax.experimental.pallas import tpu as pltpu
from jax.sharding import PartitionSpec as P

GROUP_DIM = 256
HEAD_DIM = 128
CHUNK = 256
SUB = 128
RIM = 16
HOP = 4
PIECE = 128
STEP = 16
TILE = 512
F32 = jnp.float32
BF16 = jnp.bfloat16
MESH = pl.DeviceIdType.MESH


def dot(a, b):
    return jnp.dot(a, b, preferred_element_type=F32)


def layer_kernel(
    n_sp,
    n_tp,
    tokens,
    norm_gain,
    w_pool,
    w_query,
    w_key,
    w_value,
    w_gate,
    pool_mix,
    pool_bias,
    pool_gain,
    ret_gain,
    w_out_pool,
    w_out_ret,
    out_own,
    x_in,
    tok_own,
    tok_oth,
    wts,
    wo,
    ngain,
    pmix,
    pbias,
    pgain,
    rgain,
    pv,
    pp,
    gated,
    kr,
    kd,
    qr,
    weights,
    raw,
    pool_diff,
    pool_out,
    ret,
    cosine,
    sine,
    decay,
    qdec,
    kdec,
    fresh,
    states,
    total,
    sin_buf,
    sout_buf,
    band,
    ldec,
    acc,
    part_send,
    part_recv,
    x_sem,
    w_sem,
    wo_sem,
    small_sem,
    tok_ss,
    tok_rs,
    st_send,
    st_recv,
    rim_rs,
    part_ss,
    part_rs,
):
    tp = lax.axis_index("tp")
    sp = lax.axis_index("sp")
    rows = tokens.shape[0]
    length = rows * n_tp
    width = w_query.shape[1]
    pool_width = w_pool.shape[1]
    wide = w_out_pool.shape[1]
    tiles = wide // TILE
    blocks = tokens.shape[1] // TILE
    heads = width // HEAD_DIM
    groups = pool_width // GROUP_DIM
    chunks = length // CHUNK
    per_half = rows // CHUNK
    pieces = rows // PIECE
    seq_len = length * n_sp
    own = pl.multiple_of(tp * rows, rows)
    other = pl.multiple_of((n_tp - 1 - tp) * rows, rows)
    peer = {"tp": n_tp - 1 - tp}

    gain_in = pltpu.make_async_copy(norm_gain, ngain, small_sem.at[0])
    gain_in.start()
    x_copies = []
    for i in range(pieces):
        at = pl.ds(i * PIECE, PIECE)
        x_copies.append(pltpu.make_async_copy(tokens.at[at], x_in.at[at], x_sem.at[i]))
        x_copies[i].start()
    w_in = [
        pltpu.make_async_copy(w, wts.at[i], w_sem.at[i])
        for i, w in enumerate((w_key, w_value, w_pool, w_query, w_gate))
    ]
    smalls = [
        pltpu.make_async_copy(src, dst, small_sem.at[i + 1])
        for i, (src, dst) in enumerate(
            ((pool_mix, pmix), (pool_bias, pbias), (pool_gain, pgain), (ret_gain, rgain))
        )
    ]
    wo_in = [
        pltpu.make_async_copy(
            src.at[:, pl.ds(n * TILE, TILE)],
            wo.at[n, pl.ds(low, src.shape[0])],
            wo_sem.at[i, n],
        )
        for i, (src, low) in enumerate(((w_out_pool, 0), (w_out_ret, pool_width)))
        for n in range(tiles)
    ]
    for copy in w_in:
        copy.start(priority=1)

    barrier = pltpu.get_barrier_semaphore()
    pl.semaphore_signal(barrier, inc=1, device_id=peer, device_id_type=MESH)

    @pl.when(sp > 0)
    def _():
        pl.semaphore_signal(barrier, inc=1, device_id={"sp": sp - 1}, device_id_type=MESH)

    @pl.when(sp < n_sp - 1)
    def _():
        pl.semaphore_signal(barrier, inc=1, device_id={"sp": sp + 1}, device_id_type=MESH)

    def log_decay(h):
        total_heads = heads * n_tp
        value = jnp.float32(0.0)
        for t in range(n_tp):
            one = -(2.0**-5) * (seq_len / 16.0) ** (-2.0 * (t * heads + h) / (total_heads - 1))
            value = jnp.where(tp == t, jnp.float32(one), value)
        return value

    logs = [log_decay(h) for h in range(heads)]
    lane = lax.broadcasted_iota(jnp.int32, (SUB, HEAD_DIM), 1)
    row = lax.broadcasted_iota(jnp.int32, (SUB, HEAD_DIM), 0)
    hd = HEAD_DIM // 2
    low = lane < hd
    freq = jnp.exp(
        jnp.where(low, lane, lane - hd).astype(F32) * (-math.log(10000.0) / hd)
    )
    ang = row.astype(F32) * freq
    cos_r, sin_r = jnp.cos(ang), jnp.sin(ang)
    subs = length // SUB
    base_row = lax.broadcasted_iota(jnp.int32, (subs, HEAD_DIM), 0)
    base = (sp * length + base_row * SUB).astype(F32) * freq[:subs]
    cos_b, sin_b = jnp.cos(base), jnp.sin(base)
    for b in range(subs):
        cb, sb = cos_b[b : b + 1], sin_b[b : b + 1]
        cosine[b * SUB : (b + 1) * SUB] = cb * cos_r - sb * sin_r
        s = sb * cos_r + cb * sin_r
        sine[b * SUB : (b + 1) * SUB] = jnp.where(low, -s, s)

    step_i = lax.broadcasted_iota(jnp.int32, (CHUNK, HEAD_DIM), 0).astype(F32)
    di = lax.broadcasted_iota(jnp.int32, (CHUNK, CHUNK), 0) - lax.broadcasted_iota(
        jnp.int32, (CHUNK, CHUNK), 1
    )
    dpos = jnp.maximum(di, 0).astype(F32)
    for h in range(heads):
        decay[h] = jnp.where(di >= 0, jnp.exp(logs[h] * dpos), 0.0)
        qdec[h] = jnp.exp(logs[h] * (step_i + 1.0))
        kdec[h] = jnp.exp(logs[h] * (CHUNK - 1.0 - step_i))
        ldec[h] = jnp.exp(jnp.full((8, HEAD_DIM), logs[h] * length, F32))
    bi = lax.broadcasted_iota(jnp.int32, (SUB, SUB + RIM), 0)
    bj = lax.broadcasted_iota(jnp.int32, (SUB, SUB + RIM), 1)
    back = bi + RIM - bj
    windows = [jnp.left_shift(jnp.int32(2), tp * groups + g) for g in range(groups)]
    for g in range(groups):
        band[g] = jnp.where((back >= 0) & (back < windows[g]), 1.0, 0.0).astype(BF16)

    sin_buf[heads] = jnp.zeros((HEAD_DIM, HEAD_DIM), BF16)

    @pl.when(sp == 0)
    def _():
        pp[0:RIM] = jnp.zeros((RIM, pool_width), BF16)
        sin_buf[...] = jnp.zeros_like(sin_buf)

    def tok_copy(i):
        at = pl.ds(i * PIECE, PIECE)
        return pltpu.make_async_remote_copy(
            src_ref=tok_own.at[:, at],
            dst_ref=tok_oth.at[:, at],
            send_sem=tok_ss.at[i],
            recv_sem=tok_rs.at[i],
            device_id=peer,
            device_id_type=MESH,
        )

    def norm_piece(i):
        starts = range(i * PIECE, (i + 1) * PIECE, STEP)
        scales = []
        for r in starts:
            x = x_in[r : r + STEP, :].astype(F32)
            scales.append(lax.rsqrt(jnp.mean(x * x, axis=-1, keepdims=True) + 1e-06))
        for r, scale in zip(starts, scales):
            x = x_in[r : r + STEP, :].astype(F32)
            normed = (x * scale * ngain[...]).astype(BF16)
            for n in range(blocks):
                tok_own[n, r : r + STEP, :] = normed[:, n * TILE : (n + 1) * TILE]

    def rotate(x, at):
        return x * cosine[at] + pltpu.roll(x, HEAD_DIM // 2, 1) * sine[at]

    half = blocks // 2
    own_at = [(tok_own, own, j) for j in range(per_half)]
    oth_at = [(tok_oth, other, j) for j in range(per_half)]

    def position(unit):
        return pl.multiple_of(unit[1] + unit[2] * CHUNK, CHUNK)

    def project(w, unit, lo=0, hi=blocks, res=None):
        src, _, j = unit
        mine = slice(j * CHUNK, (j + 1) * CHUNK)
        for n in range(lo, hi):
            term = dot(src[n, mine, :], wts[w, n * TILE : (n + 1) * TILE, :])
            res = term if res is None else res + term
        return res

    def split(w, unit, between):
        res = project(w, unit, 0, half)
        between()
        return project(w, unit, half, blocks, res)

    def nothing():
        pass

    def head_cols(h):
        return slice(h * HEAD_DIM, (h + 1) * HEAD_DIM)

    def key_unit(unit, between=nothing):
        at = pl.ds(position(unit), CHUNK)
        key = split(0, unit, between)
        for h in range(heads):
            k = rotate(key[:, head_cols(h)].astype(BF16).astype(F32), at) * HEAD_DIM**-0.5
            kr[at, head_cols(h)] = k.astype(BF16)
            kd[at, head_cols(h)] = (k * kdec[h]).astype(BF16)

    def value_unit(unit, between=nothing):
        pv[pl.ds(position(unit), CHUNK)] = split(1, unit, between).astype(BF16)

    def state_unit(unit):
        start = position(unit)
        at = pl.ds(start, CHUNK)
        for h in range(heads):
            fresh[start // CHUNK, h] = lax.dot_general(
                kd[at, head_cols(h)],
                pv[at, head_cols(h)],
                (((0,), (0,)), ((), ())),
                preferred_element_type=F32,
            )

    def pool_unit(unit, between=nothing):
        at = pl.ds(pl.multiple_of(position(unit) + RIM, RIM), CHUNK)
        pp[at] = split(2, unit, between).astype(BF16)

    def query_unit(unit, between=nothing):
        at = pl.ds(position(unit), CHUNK)
        q = split(3, unit, between)
        for h in range(heads):
            qr[at, head_cols(h)] = rotate(q[:, head_cols(h)].astype(BF16).astype(F32), at).astype(BF16)

    def gate_unit(unit, between=nothing):
        at = pl.ds(position(unit), CHUNK)
        g = split(4, unit, between).astype(BF16).astype(F32)
        gated[at] = g * (1.0 / (1.0 + jnp.exp(-g))) * rgain[...]

    def score_unit(unit):
        at = pl.ds(position(unit), CHUNK)
        for h in range(heads):
            scores = lax.dot_general(
                qr[at, head_cols(h)],
                kr[at, head_cols(h)],
                (((1,), (1,)), ((), ())),
                preferred_element_type=F32,
            )
            weights[h] = (scores * decay[h]).astype(BF16)

    def intra_unit(unit):
        at = pl.ds(position(unit), CHUNK)
        for h in range(heads):
            raw[at, head_cols(h)] = dot(weights[h], pv[at, head_cols(h)])

    def pool_pieces(c):
        for i in range(CHUNK // SUB):
            for g in range(groups):
                yield c * CHUNK + i * SUB, g, slice(g * GROUP_DIM, (g + 1) * GROUP_DIM)

    def pool_windows(c):
        for first, g, cols in pool_pieces(c):
            here = sp * length + first + lax.broadcasted_iota(jnp.int32, (SUB, GROUP_DIM), 0)
            span = pp[first : first + SUB + RIM, cols]
            x = pp[first + RIM : first + RIM + SUB, cols].astype(F32)
            count = jnp.minimum(here + 1, windows[g]).astype(F32)
            pool_diff[first : first + SUB, cols] = (dot(band[g], span) / count - x).astype(BF16)

    def pool_mixing(c):
        for first, g, cols in pool_pieces(c):
            mixed = dot(pool_diff[first : first + SUB, cols], pmix[g]) + pbias[g : g + 1]
            pool_out[first : first + SUB, cols] = (mixed * pgain[:, cols]).astype(BF16)

    def st_copy(h):
        return pltpu.make_async_remote_copy(
            src_ref=sout_buf.at[h],
            dst_ref=sin_buf.at[h],
            send_sem=st_send.at[h],
            recv_sem=st_recv.at[h],
            device_id={"sp": sp + 1},
            device_id_type=MESH,
        )

    rim_copy = pltpu.make_async_remote_copy(
        src_ref=pp.at[pl.ds(length, RIM)],
        dst_ref=pp.at[pl.ds(0, RIM)],
        send_sem=rim_rs.at[0],
        recv_sem=rim_rs.at[1],
        device_id={"sp": sp + 1},
        device_id_type=MESH,
    )

    def pass_on(slot, h):
        sout_buf[slot] = (total[h] + ldec[h, 0:1] * sin_buf[slot].astype(F32)).astype(BF16)

    def relay(c):
        h = c - HOP * (sp - 1)
        active = (h >= 0) & (h < heads) & (sp > 0) & (sp < n_sp - 1)
        slot = jnp.where(active, h, heads)

        @pl.when(active)
        def _():
            st_copy(h).wait_recv()

        pass_on(slot, jnp.where(active, h, 0))

        @pl.when(active)
        def _():
            st_copy(h).start()

    slots = 8

    gain_in.wait()
    x_copies[0].wait()
    norm_piece(0)
    neighbours = jnp.where(sp > 0, 1, 0) + jnp.where(sp < n_sp - 1, 1, 0)
    pl.semaphore_wait(barrier, 1 + neighbours)
    tok_copy(0).start()
    per_chunk = CHUNK // PIECE
    for i in range(1, per_chunk):
        x_copies[i].wait()
        norm_piece(i)
        tok_copy(i).start()
    for i in range(per_chunk, pieces):
        x_copies[i].wait()
    w_in[0].wait()
    for copy in smalls + wo_in:
        copy.start(priority=1)

    def late_norm():
        for i in range(per_chunk, pieces):
            norm_piece(i)

    def late_send():
        for i in range(per_chunk, pieces):
            tok_copy(i).start()

    def arrive(j):
        for i in range(j * per_chunk, (j + 1) * per_chunk):
            tok_copy(i).wait_recv()
        if j + 1 == per_half:
            for copy in w_in[2:] + smalls:
                copy.wait()

    units = own_at + oth_at
    before = None
    for i, unit in enumerate(units):
        key_unit(unit, functools.partial(state_unit, before) if i > 0 else late_norm)
        nxt = i + 1 - per_half
        if i == 0:
            w_in[1].wait()
            value_unit(unit, late_send)
        elif 0 <= nxt < per_half:
            value_unit(unit, functools.partial(arrive, nxt))
        else:
            value_unit(unit)
        before = unit

    def combine():
        state_unit(before)
        for h in range(heads):
            step = jnp.exp(jnp.full((1, HEAD_DIM), logs[h] * CHUNK, F32))
            run = fresh[0, h]
            states[0, h] = jnp.zeros((HEAD_DIM, HEAD_DIM), F32)
            for c in range(1, chunks):
                states[c, h] = run
                run = run * step + fresh[c, h]
            total[h] = run
            sout_buf[h] = run.astype(BF16)

    pool_unit(units[0], combine)

    @pl.when((sp == 0) & (sp < n_sp - 1))
    def _():
        for h in range(heads):
            st_copy(h).start()

    for unit in units[1:]:
        pool_unit(unit)

    def send_rim():
        @pl.when(sp < n_sp - 1)
        def _():
            rim_copy.start()

    query_unit(units[0], send_rim)
    query_unit(units[1], functools.partial(relay, 0))
    query_unit(units[2], functools.partial(relay, 1))
    query_unit(units[3], functools.partial(relay, 2))

    def rim_wait():
        for copy in wo_in:
            copy.wait()

        @pl.when(sp > 0)
        def _():
            rim_copy.wait_recv()

    marks = [(3,), (4, 5), (6, 7)]
    for i, unit in enumerate(units):
        c = (i + 1) % chunks

        def mid():
            for slot in marks[i] if i < len(marks) else ():
                relay(slot)
            if c == 0:
                rim_wait()
            intra_unit(unit)
            pool_windows(c)

        score_unit(unit)
        gate_unit(unit, mid)
        pool_mixing(c)
    def forward(h, carry):
        late = (h + HOP * (sp - 1) >= slots) & (sp < n_sp - 1)

        @pl.when(late)
        def _():
            st_copy(h).wait_recv()
            pass_on(h, h)
            st_copy(h).start()

        return carry

    if n_sp - 2 > slots // HOP:
        lax.fori_loop(0, heads, forward, 0)

    def last_states():
        @pl.when((sp > 0) & (sp == n_sp - 1))
        def _():
            for h in range(heads):
                st_copy(h).wait_recv()

    def pool_share(j, between=nothing):
        at = pl.ds(position(oth_at[j]), CHUNK)
        mine = slice(j * CHUNK, (j + 1) * CHUNK)
        for n in range(tiles):
            if n == tiles - 1:
                between()
            cols = slice(n * TILE, (n + 1) * TILE)
            acc[mine, cols] = dot(pool_out[at, :], wo[n, :pool_width, :])

    for j in range(per_half - 1):
        pool_share(j, last_states)
    if per_half == 1:
        last_states()

    def finish(unit):
        start = position(unit)
        at = pl.ds(start, CHUNK)
        c = start // CHUNK
        for h in range(heads):
            cols = head_cols(h)
            ahead = jnp.exp(jnp.full((1, HEAD_DIM), logs[h], F32) * start.astype(F32))
            state = (states[c, h] + sin_buf[h].astype(F32) * ahead).astype(BF16)
            r = raw[at, cols] + qdec[h] * dot(qr[at, cols], state)
            r = r - jnp.mean(r, axis=-1, keepdims=True)
            var = jnp.mean(r * r, axis=-1, keepdims=True)
            ret[at, cols] = (gated[at, cols] * (r * lax.rsqrt(var + 1e-06))).astype(BF16)

    def part_copy(j, n):
        at = pl.ds(j * CHUNK, CHUNK)
        return pltpu.make_async_remote_copy(
            src_ref=part_send.at[n, at],
            dst_ref=part_recv.at[n, at],
            send_sem=part_ss.at[j, n],
            recv_sem=part_rs.at[j, n],
            device_id=peer,
            device_id_type=MESH,
        )

    def multiply_other(j, n, between=nothing):
        at = pl.ds(position(oth_at[j]), CHUNK)
        mine = slice(j * CHUNK, (j + 1) * CHUNK)
        cols = slice(n * TILE, (n + 1) * TILE)
        cut = width // 2
        res = dot(ret[at, :cut], wo[n, pool_width : pool_width + cut, :])
        between()
        res = res + dot(ret[at, cut:], wo[n, pool_width + cut :, :])
        part_send[n, mine, :] = (acc[mine, cols] + res).astype(BF16)

    def multiply_own(j, n, between=nothing, landed=False):
        at = pl.ds(position(own_at[j]), CHUNK)
        mine = slice(j * CHUNK, (j + 1) * CHUNK)
        cols = slice(n * TILE, (n + 1) * TILE)
        res = dot(pool_out[at, :], wo[n, :pool_width, :])
        between()
        res = (res + dot(ret[at, :], wo[n, pool_width:, :])).astype(BF16)
        if landed:
            res = (res.astype(F32) + part_recv[n, mine, :].astype(F32)).astype(BF16)
        out_own[mine, cols] = res

    def add_received(j, n):
        cols = slice(n * TILE, (n + 1) * TILE)
        for r in range(j * CHUNK, (j + 1) * CHUNK, 4 * STEP):
            mine = slice(r, r + 4 * STEP)
            out_own[mine, cols] = (
                out_own[mine, cols].astype(F32) + part_recv[n, mine, :].astype(F32)
            ).astype(BF16)

    def send(j, tiles_of):
        def start():
            for n in tiles_of:
                part_copy(j, n).start()

        return start

    def land(j):
        def wait():
            for n in range(tiles):
                part_copy(j, n).wait_recv()

        return wait

    order = oth_at + own_at
    ready = tiles - 2
    finish(order[0])
    pool_share(per_half - 1)
    for i in range(len(order)):
        j = i % per_half
        last = i == len(order) - 1
        for n in range(tiles):
            between = nothing
            if n == 0 and 0 < i < per_half:
                between = send(i - 1, range(tiles))
            if n == 0 and i == per_half:
                between = send(i - 1, range(ready, tiles))
            if n == tiles - 1 and i == per_half - 1:
                between = send(i, range(ready))
            if n == 0 and i > per_half:
                between = land(j - 1)
            if n == tiles - 1 and last:
                between = land(per_half - 1)
            if i < per_half:
                multiply_other(j, n, between)
            else:
                multiply_own(j, n, between, n == tiles - 1 and last)
            if n == 0 and not last:
                finish(order[i + 1])
            if i > per_half and 0 < n < tiles - 1:
                for k in range(n - 1, tiles, tiles - 2):
                    add_received(j - 1, k)
    for n in range(tiles - 1):
        add_received(per_half - 1, n)

    for i in range(pieces):
        tok_copy(i).wait_send()
    for j in range(per_half):
        for n in range(tiles):
            part_copy(j, n).wait_send()

    @pl.when(sp < n_sp - 1)
    def _():
        rim_copy.wait_send()
        for h in range(heads):
            st_copy(h).wait_send()


def per_device(
    tokens,
    norm_gain,
    w_pool,
    w_query,
    w_key,
    w_value,
    w_gate,
    pool_mix,
    pool_bias,
    pool_gain,
    ret_gain,
    w_out_pool,
    w_out_ret,
):
    n_sp, n_tp = lax.axis_size("sp"), lax.axis_size("tp")
    rows, model = tokens.shape
    length = rows * n_tp
    width = w_query.shape[1]
    heads = width // HEAD_DIM
    pool_width = w_pool.shape[1]
    groups = pool_width // GROUP_DIM
    chunks = length // CHUNK
    per_half = rows // CHUNK
    pieces = rows // PIECE
    wide = w_out_pool.shape[1]
    hbm = pl.BlockSpec(memory_space=pltpu.HBM)
    vmem = pl.BlockSpec(memory_space=pltpu.VMEM)
    dma = pltpu.SemaphoreType.DMA
    flops = 2 * length * model * (pool_width + 4 * width) + 2 * length * (pool_width + width) * wide
    return pl.pallas_call(
        functools.partial(layer_kernel, n_sp, n_tp),
        out_shape=pltpu.VMEM((rows, wide), BF16),
        in_specs=[hbm] * 13,
        out_specs=vmem,
        scratch_shapes=[
            pltpu.VMEM((rows, model), BF16),
            pltpu.VMEM((model // TILE, rows, TILE), BF16),
            pltpu.VMEM((model // TILE, rows, TILE), BF16),
            pltpu.VMEM((5, model, width), BF16),
            pltpu.VMEM((wide // TILE, pool_width + width, TILE), BF16),
            pltpu.VMEM((1, model), F32),
            pltpu.VMEM((groups, GROUP_DIM, GROUP_DIM), BF16),
            pltpu.VMEM((groups, GROUP_DIM), F32),
            pltpu.VMEM((1, pool_width), F32),
            pltpu.VMEM((1, width), F32),
            pltpu.VMEM((length, width), BF16),
            pltpu.VMEM((length + RIM, pool_width), BF16),
            pltpu.VMEM((length, width), F32),
            pltpu.VMEM((length, width), BF16),
            pltpu.VMEM((length, width), BF16),
            pltpu.VMEM((length, width), BF16),
            pltpu.VMEM((heads, CHUNK, CHUNK), BF16),
            pltpu.VMEM((length, width), F32),
            pltpu.VMEM((length, pool_width), BF16),
            pltpu.VMEM((length, pool_width), BF16),
            pltpu.VMEM((length, width), BF16),
            pltpu.VMEM((length, HEAD_DIM), F32),
            pltpu.VMEM((length, HEAD_DIM), F32),
            pltpu.VMEM((heads, CHUNK, CHUNK), F32),
            pltpu.VMEM((heads, CHUNK, HEAD_DIM), F32),
            pltpu.VMEM((heads, CHUNK, HEAD_DIM), F32),
            pltpu.VMEM((chunks, heads, HEAD_DIM, HEAD_DIM), F32),
            pltpu.VMEM((chunks, heads, HEAD_DIM, HEAD_DIM), F32),
            pltpu.VMEM((heads, HEAD_DIM, HEAD_DIM), F32),
            pltpu.VMEM((heads + 1, HEAD_DIM, HEAD_DIM), BF16),
            pltpu.VMEM((heads + 1, HEAD_DIM, HEAD_DIM), BF16),
            pltpu.VMEM((groups, SUB, SUB + RIM), BF16),
            pltpu.VMEM((heads, 8, HEAD_DIM), F32),
            pltpu.VMEM((rows, wide), F32),
            pltpu.VMEM((wide // TILE, rows, TILE), BF16),
            pltpu.VMEM((wide // TILE, rows, TILE), BF16),
            dma((pieces,)),
            dma((5,)),
            dma((2, wide // TILE)),
            dma((5,)),
            dma((pieces,)),
            dma((pieces,)),
            dma((heads,)),
            dma((heads,)),
            dma((2,)),
            dma((per_half, wide // TILE)),
            dma((per_half, wide // TILE)),
        ],
        compiler_params=pltpu.CompilerParams(
            collective_id=0, has_side_effects=True, vmem_limit_bytes=56 * 1024 * 1024
        ),
        cost_estimate=pl.CostEstimate(
            flops=flops, bytes_accessed=20 * 1024 * 1024, transcendentals=0
        ),
    )(
        tokens,
        norm_gain.reshape(1, -1),
        w_pool,
        w_query,
        w_key,
        w_value,
        w_gate,
        pool_mix,
        pool_bias,
        pool_gain.reshape(1, -1),
        ret_gain.reshape(1, -1),
        w_out_pool,
        w_out_ret,
    )


def solution(mesh):
    return jax.shard_map(
        per_device,
        mesh=mesh,
        in_specs=(
            P(("fs", "sp", "tp"), None),
            P(),
            P(None, "tp"),
            P(None, "tp"),
            P(None, "tp"),
            P(None, "tp"),
            P(None, "tp"),
            P("tp", None, None),
            P("tp", None),
            P("tp"),
            P("tp"),
            P("tp", None),
            P("tp", None),
        ),
        out_specs=P(("fs", "sp", "tp"), None),
        check_vma=False,
    )
```

```python
import functools
import math

import jax
import jax.numpy as jnp
from jax import lax
from jax.experimental import pallas as pl
from jax.experimental.pallas import tpu as pltpu
from jax.sharding import PartitionSpec as P

GROUP_DIM = 256
HEAD_DIM = 128
CHUNK = 256
SUB = 128
RIM = 16
HOP = 4
PIECE = 128
STEP = 16
TILE = 512
F32 = jnp.float32
BF16 = jnp.bfloat16
MESH = pl.DeviceIdType.MESH


def dot(a, b):
    return jnp.dot(a, b, preferred_element_type=F32)


def layer_kernel(
    n_sp,
    n_tp,
    tokens,
    norm_gain,
    w_pool,
    w_query,
    w_key,
    w_value,
    w_gate,
    pool_mix,
    pool_bias,
    pool_gain,
    ret_gain,
    w_out_pool,
    w_out_ret,
    out_own,
    x_in,
    tok_own,
    tok_oth,
    wts,
    wo,
    ngain,
    pmix,
    pbias,
    pgain,
    rgain,
    pv,
    pp,
    gated,
    kr,
    kd,
    qr,
    weights,
    raw,
    pool_diff,
    pool_out,
    ret,
    cosine,
    sine,
    decay,
    qdec,
    kdec,
    fresh,
    states,
    total,
    sin_buf,
    sout_buf,
    band,
    ldec,
    acc,
    part_send,
    part_recv,
    x_sem,
    key_sem,
    w_sem,
    wo_sem,
    small_sem,
    tok_ss,
    tok_rs,
    st_send,
    st_recv,
    rim_rs,
    part_ss,
    part_rs,
):
    tp = lax.axis_index("tp")
    sp = lax.axis_index("sp")
    rows = tokens.shape[0]
    length = rows * n_tp
    width = w_query.shape[1]
    pool_width = w_pool.shape[1]
    wide = w_out_pool.shape[1]
    tiles = wide // TILE
    blocks = tokens.shape[1] // TILE
    heads = width // HEAD_DIM
    groups = pool_width // GROUP_DIM
    chunks = length // CHUNK
    per_half = rows // CHUNK
    pieces = rows // PIECE
    seq_len = length * n_sp
    own = pl.multiple_of(tp * rows, rows)
    other = pl.multiple_of((n_tp - 1 - tp) * rows, rows)
    peer = {"tp": n_tp - 1 - tp}

    gain_in = pltpu.make_async_copy(norm_gain, ngain, small_sem.at[0])
    gain_in.start()
    x_copies = []
    for i in range(pieces):
        at = pl.ds(i * PIECE, PIECE)
        x_copies.append(pltpu.make_async_copy(tokens.at[at], x_in.at[at], x_sem.at[i]))
        x_copies[i].start()
    deep = w_key.shape[0] // 2
    key_in = [
        pltpu.make_async_copy(
            w_key.at[pl.ds(i * deep, deep)], wts.at[0, pl.ds(i * deep, deep)], key_sem.at[i]
        )
        for i in range(2)
    ]
    w_in = key_in[:1] + [
        pltpu.make_async_copy(w, wts.at[i + 1], w_sem.at[i])
        for i, w in enumerate((w_value, w_pool, w_query, w_gate))
    ]
    smalls = [
        pltpu.make_async_copy(src, dst, small_sem.at[i + 1])
        for i, (src, dst) in enumerate(
            ((pool_mix, pmix), (pool_bias, pbias), (pool_gain, pgain), (ret_gain, rgain))
        )
    ]
    wo_in = [
        pltpu.make_async_copy(
            src.at[:, pl.ds(n * TILE, TILE)],
            wo.at[n, pl.ds(low, src.shape[0])],
            wo_sem.at[i, n],
        )
        for i, (src, low) in enumerate(((w_out_pool, 0), (w_out_ret, pool_width)))
        for n in range(tiles)
    ]
    for copy in key_in + w_in[1:]:
        copy.start(priority=1)

    barrier = pltpu.get_barrier_semaphore()
    pl.semaphore_signal(barrier, inc=1, device_id=peer, device_id_type=MESH)

    @pl.when(sp > 0)
    def _():
        pl.semaphore_signal(barrier, inc=1, device_id={"sp": sp - 1}, device_id_type=MESH)

    @pl.when(sp < n_sp - 1)
    def _():
        pl.semaphore_signal(barrier, inc=1, device_id={"sp": sp + 1}, device_id_type=MESH)

    def log_decay(h):
        total_heads = heads * n_tp
        value = jnp.float32(0.0)
        for t in range(n_tp):
            one = -(2.0**-5) * (seq_len / 16.0) ** (-2.0 * (t * heads + h) / (total_heads - 1))
            value = jnp.where(tp == t, jnp.float32(one), value)
        return value

    logs = [log_decay(h) for h in range(heads)]
    lane = lax.broadcasted_iota(jnp.int32, (SUB, HEAD_DIM), 1)
    row = lax.broadcasted_iota(jnp.int32, (SUB, HEAD_DIM), 0)
    hd = HEAD_DIM // 2
    low = lane < hd
    freq = jnp.exp(
        jnp.where(low, lane, lane - hd).astype(F32) * (-math.log(10000.0) / hd)
    )
    ang = row.astype(F32) * freq
    cos_r, sin_r = jnp.cos(ang), jnp.sin(ang)
    subs = length // SUB
    base_row = lax.broadcasted_iota(jnp.int32, (subs, HEAD_DIM), 0)
    base = (sp * length + base_row * SUB).astype(F32) * freq[:subs]
    cos_b, sin_b = jnp.cos(base), jnp.sin(base)
    for b in range(subs):
        cb, sb = cos_b[b : b + 1], sin_b[b : b + 1]
        cosine[b * SUB : (b + 1) * SUB] = cb * cos_r - sb * sin_r
        s = sb * cos_r + cb * sin_r
        sine[b * SUB : (b + 1) * SUB] = jnp.where(low, -s, s)

    step_i = lax.broadcasted_iota(jnp.int32, (CHUNK, HEAD_DIM), 0).astype(F32)
    di = lax.broadcasted_iota(jnp.int32, (CHUNK, CHUNK), 0) - lax.broadcasted_iota(
        jnp.int32, (CHUNK, CHUNK), 1
    )
    dpos = jnp.maximum(di, 0).astype(F32)
    for h in range(heads):
        decay[h] = jnp.where(di >= 0, jnp.exp(logs[h] * dpos), 0.0)
        qdec[h] = jnp.exp(logs[h] * (step_i + 1.0))
        kdec[h] = jnp.exp(logs[h] * (CHUNK - 1.0 - step_i))
        ldec[h] = jnp.exp(jnp.full((8, HEAD_DIM), logs[h] * length, F32))
    bi = lax.broadcasted_iota(jnp.int32, (SUB, SUB + RIM), 0)
    bj = lax.broadcasted_iota(jnp.int32, (SUB, SUB + RIM), 1)
    back = bi + RIM - bj
    windows = [jnp.left_shift(jnp.int32(2), tp * groups + g) for g in range(groups)]
    for g in range(groups):
        band[g] = jnp.where((back >= 0) & (back < windows[g]), 1.0, 0.0).astype(BF16)

    sin_buf[heads] = jnp.zeros((HEAD_DIM, HEAD_DIM), BF16)

    @pl.when(sp == 0)
    def _():
        pp[0:RIM] = jnp.zeros((RIM, pool_width), BF16)
        sin_buf[...] = jnp.zeros_like(sin_buf)

    def tok_copy(i):
        at = pl.ds(i * PIECE, PIECE)
        return pltpu.make_async_remote_copy(
            src_ref=tok_own.at[:, at],
            dst_ref=tok_oth.at[:, at],
            send_sem=tok_ss.at[i],
            recv_sem=tok_rs.at[i],
            device_id=peer,
            device_id_type=MESH,
        )

    def norm_piece(i):
        starts = range(i * PIECE, (i + 1) * PIECE, STEP)
        scales = []
        for r in starts:
            x = x_in[r : r + STEP, :].astype(F32)
            scales.append(lax.rsqrt(jnp.mean(x * x, axis=-1, keepdims=True) + 1e-06))
        for r, scale in zip(starts, scales):
            x = x_in[r : r + STEP, :].astype(F32)
            normed = (x * scale * ngain[...]).astype(BF16)
            for n in range(blocks):
                tok_own[n, r : r + STEP, :] = normed[:, n * TILE : (n + 1) * TILE]

    def rotate(x, at):
        return x * cosine[at] + pltpu.roll(x, HEAD_DIM // 2, 1) * sine[at]

    half = blocks // 2
    own_at = [(tok_own, own, j) for j in range(per_half)]
    oth_at = [(tok_oth, other, j) for j in range(per_half)]

    def span_of(unit):
        return unit[3] if len(unit) > 3 else CHUNK

    def position(unit):
        return pl.multiple_of(unit[1] + unit[2] * CHUNK, CHUNK)

    def project(w, unit, lo=0, hi=blocks, res=None):
        src, _, j = unit[:3]
        mine = slice(j * CHUNK, j * CHUNK + span_of(unit))
        for n in range(lo, hi):
            term = dot(src[n, mine, :], wts[w, n * TILE : (n + 1) * TILE, :])
            res = term if res is None else res + term
        return res

    def nothing():
        pass

    def split(w, unit, between):
        res = project(w, unit, 0, half)
        between()
        return project(w, unit, half, blocks, res)

    def head_cols(h):
        return slice(h * HEAD_DIM, (h + 1) * HEAD_DIM)

    def key_unit(unit, between=nothing):
        at = pl.ds(position(unit), CHUNK)
        key = split(0, unit, between)
        for h in range(heads):
            k = rotate(key[:, head_cols(h)].astype(BF16).astype(F32), at) * HEAD_DIM**-0.5
            kr[at, head_cols(h)] = k.astype(BF16)
            kd[at, head_cols(h)] = (k * kdec[h]).astype(BF16)

    def value_unit(unit, between=nothing):
        pv[pl.ds(position(unit), CHUNK)] = split(1, unit, between).astype(BF16)

    def state_unit(unit):
        start = position(unit)
        at = pl.ds(start, CHUNK)
        for h in range(heads):
            fresh[start // CHUNK, h] = lax.dot_general(
                kd[at, head_cols(h)],
                pv[at, head_cols(h)],
                (((0,), (0,)), ((), ())),
                preferred_element_type=F32,
            )

    def pool_unit(unit, between=nothing):
        at = pl.ds(pl.multiple_of(position(unit) + RIM, RIM), span_of(unit))
        pp[at] = split(2, unit, between).astype(BF16)

    def query_unit(unit, between=nothing):
        at = pl.ds(position(unit), span_of(unit))
        q = split(3, unit, between)
        for h in range(heads):
            qr[at, head_cols(h)] = rotate(q[:, head_cols(h)].astype(BF16).astype(F32), at).astype(BF16)

    def gate_unit(unit, between=nothing):
        at = pl.ds(position(unit), CHUNK)
        g = split(4, unit, between).astype(BF16).astype(F32)
        gated[at] = g * (1.0 / (1.0 + jnp.exp(-g))) * rgain[...]

    def score_unit(unit):
        at = pl.ds(position(unit), CHUNK)
        for h in range(heads):
            scores = lax.dot_general(
                qr[at, head_cols(h)],
                kr[at, head_cols(h)],
                (((1,), (1,)), ((), ())),
                preferred_element_type=F32,
            )
            weights[h] = (scores * decay[h]).astype(BF16)

    def intra_unit(unit):
        at = pl.ds(position(unit), CHUNK)
        for h in range(heads):
            raw[at, head_cols(h)] = dot(weights[h], pv[at, head_cols(h)])

    def pool_pieces(c):
        for i in range(CHUNK // SUB):
            for g in range(groups):
                yield c * CHUNK + i * SUB, g, slice(g * GROUP_DIM, (g + 1) * GROUP_DIM)

    def pool_windows(c):
        for first, g, cols in pool_pieces(c):
            here = sp * length + first + lax.broadcasted_iota(jnp.int32, (SUB, GROUP_DIM), 0)
            span = pp[first : first + SUB + RIM, cols]
            x = pp[first + RIM : first + RIM + SUB, cols].astype(F32)
            count = jnp.minimum(here + 1, windows[g]).astype(F32)
            pool_diff[first : first + SUB, cols] = (dot(band[g], span) / count - x).astype(BF16)

    def pool_mixing(c):
        for first, g, cols in pool_pieces(c):
            mixed = dot(pool_diff[first : first + SUB, cols], pmix[g]) + pbias[g : g + 1]
            pool_out[first : first + SUB, cols] = (mixed * pgain[:, cols]).astype(BF16)

    def st_copy(h):
        return pltpu.make_async_remote_copy(
            src_ref=sout_buf.at[h],
            dst_ref=sin_buf.at[h],
            send_sem=st_send.at[h],
            recv_sem=st_recv.at[h],
            device_id={"sp": sp + 1},
            device_id_type=MESH,
        )

    rim_copy = pltpu.make_async_remote_copy(
        src_ref=pp.at[pl.ds(length, RIM)],
        dst_ref=pp.at[pl.ds(0, RIM)],
        send_sem=rim_rs.at[0],
        recv_sem=rim_rs.at[1],
        device_id={"sp": sp + 1},
        device_id_type=MESH,
    )

    def pass_on(slot, h):
        sout_buf[slot] = (total[h] + ldec[h, 0:1] * sin_buf[slot].astype(F32)).astype(BF16)

    def relay(c):
        h = c - HOP * (sp - 1)
        active = (h >= 0) & (h < heads) & (sp > 0) & (sp < n_sp - 1)
        slot = jnp.where(active, h, heads)

        @pl.when(active)
        def _():
            st_copy(h).wait_recv()

        pass_on(slot, jnp.where(active, h, 0))

        @pl.when(active)
        def _():
            st_copy(h).start()

    slots = 8

    gain_in.wait()
    x_copies[0].wait()
    norm_piece(0)
    neighbours = jnp.where(sp > 0, 1, 0) + jnp.where(sp < n_sp - 1, 1, 0)
    pl.semaphore_wait(barrier, 1 + neighbours)
    tok_copy(0).start()
    per_chunk = CHUNK // PIECE
    for i in range(1, per_chunk):
        x_copies[i].wait()
        norm_piece(i)
        tok_copy(i).start()
    for i in range(per_chunk, pieces):
        x_copies[i].wait()
    key_in[0].wait()
    for copy in smalls + wo_in:
        copy.start(priority=1)

    def late_norm():
        key_in[1].wait()
        for i in range(per_chunk, pieces):
            norm_piece(i)

    def late_send():
        for i in range(per_chunk, pieces):
            tok_copy(i).start()

    def arrive(j):
        for i in range(j * per_chunk, (j + 1) * per_chunk):
            tok_copy(i).wait_recv()
        if j + 1 == per_half:
            for copy in w_in[2:] + smalls:
                copy.wait()

    units = own_at + oth_at
    before = None
    for i, unit in enumerate(units):
        key_unit(unit, functools.partial(state_unit, before) if i > 0 else late_norm)
        nxt = i + 1 - per_half
        if i == 0:
            w_in[1].wait()
            value_unit(unit, late_send)
        elif 0 <= nxt < per_half:
            value_unit(unit, functools.partial(arrive, nxt))
        else:
            value_unit(unit)
        before = unit

    def combine():
        state_unit(before)
        for h in range(heads):
            step = jnp.exp(jnp.full((1, HEAD_DIM), logs[h] * CHUNK, F32))
            run = fresh[0, h]
            states[0, h] = jnp.zeros((HEAD_DIM, HEAD_DIM), F32)
            for c in range(1, chunks):
                states[c, h] = run
                run = run * step + fresh[c, h]
            total[h] = run
            sout_buf[h] = run.astype(BF16)

    pool_unit(units[0], combine)

    @pl.when((sp == 0) & (sp < n_sp - 1))
    def _():
        for h in range(heads):
            st_copy(h).start()

    for unit in units[1:per_half]:
        pool_unit(unit)
    pool_unit((tok_oth, other, 0, rows))

    def send_rim():
        @pl.when(sp < n_sp - 1)
        def _():
            rim_copy.start()

    query_unit(units[0], send_rim)
    query_unit(units[1], functools.partial(relay, 0))
    query_unit(units[2], functools.partial(relay, 1))
    query_unit(units[3], functools.partial(relay, 2))

    def rim_wait():
        for copy in wo_in:
            copy.wait()

        @pl.when(sp > 0)
        def _():
            rim_copy.wait_recv()

    marks = [(3,), (4, 5), (6, 7)]
    for i, unit in enumerate(units):
        c = (i + 1) % chunks

        def mid():
            for slot in marks[i] if i < len(marks) else ():
                relay(slot)
            if c == 0:
                rim_wait()
            intra_unit(unit)
            pool_windows(c)

        score_unit(unit)
        gate_unit(unit, mid)
        pool_mixing(c)
    def forward(h, carry):
        late = (h + HOP * (sp - 1) >= slots) & (sp < n_sp - 1)

        @pl.when(late)
        def _():
            st_copy(h).wait_recv()
            pass_on(h, h)
            st_copy(h).start()

        return carry

    if n_sp - 2 > slots // HOP:
        lax.fori_loop(0, heads, forward, 0)

    def last_states():
        @pl.when((sp > 0) & (sp == n_sp - 1))
        def _():
            for h in range(heads):
                st_copy(h).wait_recv()

    def pool_share(j, between=nothing):
        at = pl.ds(position(oth_at[j]), CHUNK)
        mine = slice(j * CHUNK, (j + 1) * CHUNK)
        for n in range(tiles):
            if n == 1:
                between()
            cols = slice(n * TILE, (n + 1) * TILE)
            acc[mine, cols] = dot(pool_out[at, :], wo[n, :pool_width, :])

    def finish(unit):
        start = position(unit)
        at = pl.ds(start, CHUNK)
        c = start // CHUNK
        for h in range(heads):
            cols = head_cols(h)
            ahead = jnp.exp(jnp.full((1, HEAD_DIM), logs[h], F32) * start.astype(F32))
            state = (states[c, h] + sin_buf[h].astype(F32) * ahead).astype(BF16)
            r = raw[at, cols] + qdec[h] * dot(qr[at, cols], state)
            r = r - jnp.mean(r, axis=-1, keepdims=True)
            var = jnp.mean(r * r, axis=-1, keepdims=True)
            ret[at, cols] = (gated[at, cols] * (r * lax.rsqrt(var + 1e-06))).astype(BF16)

    def part_copy(j, n):
        at = pl.ds(j * CHUNK, CHUNK)
        return pltpu.make_async_remote_copy(
            src_ref=part_send.at[n, at],
            dst_ref=part_recv.at[n, at],
            send_sem=part_ss.at[j, n],
            recv_sem=part_rs.at[j, n],
            device_id=peer,
            device_id_type=MESH,
        )

    def multiply_other(j, n, between=nothing):
        at = pl.ds(position(oth_at[j]), CHUNK)
        mine = slice(j * CHUNK, (j + 1) * CHUNK)
        cols = slice(n * TILE, (n + 1) * TILE)
        cut = width // 2
        res = dot(ret[at, :cut], wo[n, pool_width : pool_width + cut, :])
        between()
        res = res + dot(ret[at, cut:], wo[n, pool_width + cut :, :])
        part_send[n, mine, :] = (acc[mine, cols] + res).astype(BF16)

    def multiply_own(j, n, between=nothing, landed=False):
        at = pl.ds(position(own_at[j]), CHUNK)
        mine = slice(j * CHUNK, (j + 1) * CHUNK)
        cols = slice(n * TILE, (n + 1) * TILE)
        res = dot(pool_out[at, :], wo[n, :pool_width, :])
        between()
        res = (res + dot(ret[at, :], wo[n, pool_width:, :])).astype(BF16)
        if landed:
            res = (res.astype(F32) + part_recv[n, mine, :].astype(F32)).astype(BF16)
        out_own[mine, cols] = res

    def add_received(j, n):
        cols = slice(n * TILE, (n + 1) * TILE)
        for r in range(j * CHUNK, (j + 1) * CHUNK, 4 * STEP):
            mine = slice(r, r + 4 * STEP)
            out_own[mine, cols] = (
                out_own[mine, cols].astype(F32) + part_recv[n, mine, :].astype(F32)
            ).astype(BF16)

    def send(j, tiles_of):
        def start():
            for n in tiles_of:
                part_copy(j, n).start()

        return start

    def land(j):
        def wait():
            for n in range(tiles):
                part_copy(j, n).wait_recv()

        return wait

    order = oth_at + own_at
    ready = tiles - 2

    def begin():
        last_states()
        finish(order[0])

    for k in range(per_half):
        pool_share(k, begin if k == per_half - 1 else nothing)
    for i in range(len(order)):
        j = i % per_half
        last = i == len(order) - 1
        for n in range(tiles):
            between = nothing
            if n == 0 and 0 < i < per_half:
                between = send(i - 1, range(tiles))
            if n == 0 and i == per_half:
                between = send(i - 1, range(ready, tiles))
            if n == tiles - 1 and i == per_half - 1:
                between = send(i, range(ready))
            if n == 0 and i > per_half:
                between = land(j - 1)
            if n == tiles - 1 and last:
                between = land(per_half - 1)
            if i < per_half:
                multiply_other(j, n, between)
            else:
                multiply_own(j, n, between, n == tiles - 1 and last)
            if n == 0 and not last:
                finish(order[i + 1])
            if i > per_half and 0 < n < tiles - 1:
                for k in range(n - 1, tiles, tiles - 2):
                    add_received(j - 1, k)
    for n in range(tiles - 1):
        add_received(per_half - 1, n)

    for i in range(pieces):
        tok_copy(i).wait_send()
    for j in range(per_half):
        for n in range(tiles):
            part_copy(j, n).wait_send()

    @pl.when(sp < n_sp - 1)
    def _():
        rim_copy.wait_send()
        for h in range(heads):
            st_copy(h).wait_send()


def per_device(
    tokens,
    norm_gain,
    w_pool,
    w_query,
    w_key,
    w_value,
    w_gate,
    pool_mix,
    pool_bias,
    pool_gain,
    ret_gain,
    w_out_pool,
    w_out_ret,
):
    n_sp, n_tp = lax.axis_size("sp"), lax.axis_size("tp")
    rows, model = tokens.shape
    length = rows * n_tp
    width = w_query.shape[1]
    heads = width // HEAD_DIM
    pool_width = w_pool.shape[1]
    groups = pool_width // GROUP_DIM
    chunks = length // CHUNK
    per_half = rows // CHUNK
    pieces = rows // PIECE
    wide = w_out_pool.shape[1]
    hbm = pl.BlockSpec(memory_space=pltpu.HBM)
    vmem = pl.BlockSpec(memory_space=pltpu.VMEM)
    dma = pltpu.SemaphoreType.DMA
    flops = 2 * length * model * (pool_width + 4 * width) + 2 * length * (pool_width + width) * wide
    return pl.pallas_call(
        functools.partial(layer_kernel, n_sp, n_tp),
        out_shape=pltpu.VMEM((rows, wide), BF16),
        in_specs=[hbm] * 13,
        out_specs=vmem,
        scratch_shapes=[
            pltpu.VMEM((rows, model), BF16),
            pltpu.VMEM((model // TILE, rows, TILE), BF16),
            pltpu.VMEM((model // TILE, rows, TILE), BF16),
            pltpu.VMEM((5, model, width), BF16),
            pltpu.VMEM((wide // TILE, pool_width + width, TILE), BF16),
            pltpu.VMEM((1, model), F32),
            pltpu.VMEM((groups, GROUP_DIM, GROUP_DIM), BF16),
            pltpu.VMEM((groups, GROUP_DIM), F32),
            pltpu.VMEM((1, pool_width), F32),
            pltpu.VMEM((1, width), F32),
            pltpu.VMEM((length, width), BF16),
            pltpu.VMEM((length + RIM, pool_width), BF16),
            pltpu.VMEM((length, width), F32),
            pltpu.VMEM((length, width), BF16),
            pltpu.VMEM((length, width), BF16),
            pltpu.VMEM((length, width), BF16),
            pltpu.VMEM((heads, CHUNK, CHUNK), BF16),
            pltpu.VMEM((length, width), F32),
            pltpu.VMEM((length, pool_width), BF16),
            pltpu.VMEM((length, pool_width), BF16),
            pltpu.VMEM((length, width), BF16),
            pltpu.VMEM((length, HEAD_DIM), F32),
            pltpu.VMEM((length, HEAD_DIM), F32),
            pltpu.VMEM((heads, CHUNK, CHUNK), F32),
            pltpu.VMEM((heads, CHUNK, HEAD_DIM), F32),
            pltpu.VMEM((heads, CHUNK, HEAD_DIM), F32),
            pltpu.VMEM((chunks, heads, HEAD_DIM, HEAD_DIM), F32),
            pltpu.VMEM((chunks, heads, HEAD_DIM, HEAD_DIM), F32),
            pltpu.VMEM((heads, HEAD_DIM, HEAD_DIM), F32),
            pltpu.VMEM((heads + 1, HEAD_DIM, HEAD_DIM), BF16),
            pltpu.VMEM((heads + 1, HEAD_DIM, HEAD_DIM), BF16),
            pltpu.VMEM((groups, SUB, SUB + RIM), BF16),
            pltpu.VMEM((heads, 8, HEAD_DIM), F32),
            pltpu.VMEM((rows, wide), F32),
            pltpu.VMEM((wide // TILE, rows, TILE), BF16),
            pltpu.VMEM((wide // TILE, rows, TILE), BF16),
            dma((pieces,)),
            dma((2,)),
            dma((4,)),
            dma((2, wide // TILE)),
            dma((5,)),
            dma((pieces,)),
            dma((pieces,)),
            dma((heads,)),
            dma((heads,)),
            dma((2,)),
            dma((per_half, wide // TILE)),
            dma((per_half, wide // TILE)),
        ],
        compiler_params=pltpu.CompilerParams(
            collective_id=0, has_side_effects=True, vmem_limit_bytes=56 * 1024 * 1024
        ),
        cost_estimate=pl.CostEstimate(
            flops=flops, bytes_accessed=20 * 1024 * 1024, transcendentals=0
        ),
    )(
        tokens,
        norm_gain.reshape(1, -1),
        w_pool,
        w_query,
        w_key,
        w_value,
        w_gate,
        pool_mix,
        pool_bias,
        pool_gain.reshape(1, -1),
        ret_gain.reshape(1, -1),
        w_out_pool,
        w_out_ret,
    )


def solution(mesh):
    return jax.shard_map(
        per_device,
        mesh=mesh,
        in_specs=(
            P(("fs", "sp", "tp"), None),
            P(),
            P(None, "tp"),
            P(None, "tp"),
            P(None, "tp"),
            P(None, "tp"),
            P(None, "tp"),
            P("tp", None, None),
            P("tp", None),
            P("tp"),
            P("tp"),
            P("tp", None),
            P("tp", None),
        ),
        out_specs=P(("fs", "sp", "tp"), None),
        check_vma=False,
    )
```
